256 devices in a mesh: grp: 2 (over y), sp: 16 (over z), fs: 4 (over x), tp: 2 (over core).
Axes of the slice: x: 4, y: 2, z: 16, core: 2. Of those that a mesh axis runs over, the one named last changes fastest.
The devices are a block of a 4x16x16 slice.
Arguments:
- tokens: bfloat16 [16, 2048, 2048], P(('grp', 'fs'), ('sp', 'tp')), parts along dimension 0, may hold values from -24 to 24
- norm_gain: float32 [2048], replicated, may hold values from 0.1 to 1.9
- w_query: bfloat16 [2048, 1024], P(('sp', 'fs'), 'tp'), may hold values from -0.125 to 0.125
- w_key: bfloat16 [2048, 1024], P(('sp', 'fs'), 'tp'), may hold values from -0.125 to 0.125
- w_value: bfloat16 [2048, 1024], P(('sp', 'fs'), 'tp'), may hold values from -0.125 to 0.125
- query_gain: float32 [1024], P('tp'), may hold values from 1 to 26
- key_gain: float32 [1024], P('tp'), may hold values from 0.1 to 1.9
- mix_lambda: float32 [8], P('tp'), may hold values from 0.3 to 0.8
- head_gain: float32 [128], replicated, may hold values from 0.1 to 1.9
- w_gate_b: bfloat16 [2048, 1024], P(('sp', 'fs'), 'tp'), may hold values from -0.125 to 0.125
- w_gate_c: bfloat16 [2048, 1024], P(('sp', 'fs'), 'tp'), may hold values from -0.125 to 0.125
- w_conv_in: bfloat16 [2048, 1024], P(('sp', 'fs'), 'tp'), may hold values from -0.125 to 0.125
- conv_taps: float32 [3, 1024], P(None, 'tp'), may hold values from -3 to 3
- w_out_attn: bfloat16 [1024, 2048], P('tp', ('sp', 'fs')), may hold values from -0.125 to 0.125
- w_out_conv: bfloat16 [1024, 2048], P('tp', ('sp', 'fs')), may hold values from -0.125 to 0.125
Outputs:
- mixed: bfloat16 [16, 2048, 2048], P(('grp', 'fs'), ('sp', 'tp')), parts along dimension 0
The draws below stay inside these ranges and needn't reach their ends.
There are 2 independent parts, one for each index of `grp`. The reference program is written for one: setup_inputs(seed, part) draws one part's arguments, and reference() takes and returns one part's arrays. A program takes and returns all parts, laid end to end along the dimension named above; an argument that names none is the same for every part. Nothing has to cross between parts.
All inputs are finite; a program needn't handle non-finite values.
Results may differ from the reference program's by a relative error of at most 0.04.
Values may be sent and summed in bfloat16 or wider, within the bound.
A program may use at most 128 MiB of HBM per device.

```python
import math
import jax
import jax.numpy as jnp
from jax import lax

D = 2048
HEADS = 8
DK = 64
DV = 128
CW = 1024
KW = 3
SEQ_LEN = 2048
SEQS = 8


def draw_tokens(key, part):
    first, second, third = jax.random.split(jax.random.fold_in(key, 11), 3)
    shape = (SEQS, SEQ_LEN, D)
    base = jnp.clip(jax.random.normal(first, shape, jnp.float32), -4.0, 4.0)
    row_scale = jnp.exp(jax.random.uniform(second, (SEQS, SEQ_LEN, 1), jnp.float32, math.log(0.3), math.log(3.0)))
    col_scale = jnp.exp(jax.random.uniform(third, (1, 1, D), jnp.float32, math.log(0.5), math.log(2.0)))
    return (base * row_scale * col_scale).astype(jnp.bfloat16)


def draw_query_gain(key, part):
    first = jax.random.fold_in(jax.random.fold_in(key, 23), 0)
    base = 1.7 * jnp.exp(jax.random.uniform(first, (HEADS, 2, DK), jnp.float32, -0.25, 0.25))
    return base.reshape(HEADS * 2 * DK).astype(jnp.float32)


def block_scale(rng, dims, shards, smallest, high):
    loudness, own = 1.0, jax.random.fold_in(rng, 6)
    for dim, shards_of in shards:
        steps = jnp.exp(jax.random.uniform(jax.random.fold_in(own, dim), (shards_of,), jnp.float32, smallest / len(shards), high / len(shards)))
        loudness = loudness * jnp.repeat(steps, dims[dim] // shards_of).reshape([-1 if axis == dim else 1 for axis in range(len(dims))])
    return loudness


def normal_values(key, shape, spread, bound, pieces=(), held_as=jnp.bfloat16):
    array = jax.random.normal(key, shape, jnp.float32) * spread
    if len(pieces) > 0:
        array = block_scale(key, shape, pieces, -0.22, 0.18) * array
    return jnp.clip(array, min=-bound, max=bound).astype(held_as)


def setup_inputs(seed: int = 0, part: int = 0) -> dict:
    keys = jax.random.split(jax.random.key(seed), 16)
    part_splits = jax.random.split(jax.random.fold_in(keys[15], part), 16)
    tokens = draw_tokens(jax.random.fold_in(jax.random.fold_in(keys[15], part), 71), part)
    norm_gain = jnp.clip(1.0 + 0.18 * jax.random.normal(keys[1], (D,), jnp.float32), 0.1, 1.9)
    w_query = normal_values(keys[2], (D, HEADS * 2 * DK), D ** -0.5, 0.125, ((0, 64), (1, 2)))
    w_key = normal_values(keys[3], (D, HEADS * 2 * DK), D ** -0.5, 0.125, ((0, 64), (1, 2)))
    w_value = normal_values(keys[4], (D, HEADS * DV), D ** -0.5, 0.125, ((0, 64), (1, 2)))
    query_gain = draw_query_gain(jax.random.fold_in(keys[15], 71), part)
    key_gain = jnp.clip(1.0 + 0.18 * jax.random.normal(keys[6], (HEADS * 2 * DK,), jnp.float32), 0.1, 1.9)
    mix_lambda = jnp.clip(0.3 + 0.5 * jax.random.uniform(keys[7], (HEADS,), jnp.float32) ** block_scale(keys[7], (HEADS,), ((0, 2),), -0.2, 0.2), 0.3, 0.8)
    head_gain = jnp.clip(1.0 + 0.18 * jax.random.normal(keys[8], (DV,), jnp.float32), 0.1, 1.9)
    w_gate_b = normal_values(keys[9], (D, CW), D ** -0.5, 0.125, ((0, 64), (1, 2)))
    w_gate_c = normal_values(keys[10], (D, CW), D ** -0.5, 0.125, ((0, 64), (1, 2)))
    w_conv_in = normal_values(keys[11], (D, CW), D ** -0.5, 0.125, ((0, 64), (1, 2)))
    conv_taps = normal_values(keys[12], (KW, CW), 0.577, 3.0, ((1, 2),), jnp.float32)
    w_out_attn = normal_values(keys[13], (HEADS * DV, D), (HEADS * DV + CW) ** -0.5, 0.125, ((0, 2), (1, 64)))
    w_out_conv = normal_values(keys[14], (CW, D), (HEADS * DV + CW) ** -0.5, 0.125, ((0, 2), (1, 64)))
    return dict(tokens=tokens, norm_gain=norm_gain, w_query=w_query, w_key=w_key, w_value=w_value, query_gain=query_gain, key_gain=key_gain, mix_lambda=mix_lambda, head_gain=head_gain, w_gate_b=w_gate_b, w_gate_c=w_gate_c, w_conv_in=w_conv_in, conv_taps=conv_taps, w_out_attn=w_out_attn, w_out_conv=w_out_conv)


EPS = 1e-06
NEG = -1e+30
OUT_SCALE = 0.8

def rms_scale(values, gain):
    wide = values.astype(jnp.float32)
    return wide * lax.rsqrt(lax.optimization_barrier(jnp.mean(wide * wide, axis=-1, keepdims=True)) + EPS) * gain.astype(jnp.float32)

def reference(tokens, norm_gain, w_query, w_key, w_value, query_gain, key_gain, mix_lambda, head_gain, w_gate_b, w_gate_c, w_conv_in, conv_taps, w_out_attn, w_out_conv):
    length = SEQ_LEN
    block = math.gcd(length, 512)

    def one(seq):
        normed = rms_scale(seq, norm_gain).astype(jnp.bfloat16)

        def project(weight):
            return jnp.dot(normed, weight, preferred_element_type=jnp.float32).astype(jnp.bfloat16)
        query = rms_scale(project(w_query).reshape(length, HEADS, 2, DK), query_gain.reshape(HEADS, 2, DK)).astype(jnp.bfloat16)
        key = rms_scale(project(w_key).reshape(length, HEADS, 2, DK), key_gain.reshape(HEADS, 2, DK)).astype(jnp.bfloat16)
        value = project(w_value).reshape(length, HEADS, DV)
        key_wide = key.astype(jnp.float32)
        value_wide = value.astype(jnp.float32)
        key_pos = jnp.arange(length, dtype=jnp.int32)

        def attend(start):
            q_block = lax.dynamic_slice_in_dim(query, start, block, 0).astype(jnp.float32)
            q_pos = start + jnp.arange(block, dtype=jnp.int32)
            score = jnp.einsum('qhmd,khmd->hmqk', q_block, key_wide) * DK ** (-0.5)
            allowed = key_pos[None, :] <= q_pos[:, None]
            score = jnp.where(allowed, score, NEG)
            top = lax.optimization_barrier(jnp.max(score, axis=-1, keepdims=True))
            weights = jnp.exp(score - top)
            total = lax.optimization_barrier(jnp.sum(weights, axis=-1))
            rounded = lax.optimization_barrier(weights.astype(jnp.bfloat16)).astype(jnp.float32)
            summed = jnp.einsum('hmqk,khd->hmqd', rounded, value_wide)
            head_map = summed / total[..., None]
            differ = head_map[:, 0] - mix_lambda.astype(jnp.float32)[:, None, None] * head_map[:, 1]
            normal = rms_scale(differ, head_gain) * OUT_SCALE
            return normal.transpose(1, 0, 2).reshape(block, HEADS * DV).astype(jnp.bfloat16)
        starts = jnp.arange(length // block, dtype=jnp.int32) * block
        attn = lax.map(attend, starts).reshape(length, HEADS * DV)
        gate_b = project(w_gate_b)
        gate_c = project(w_gate_c)
        conv_in = project(w_conv_in)
        shaped = (gate_c.astype(jnp.float32) * conv_in.astype(jnp.float32)).astype(jnp.bfloat16)
        padded = jnp.concatenate([jnp.zeros((KW - 1, CW), jnp.bfloat16), shaped], axis=0).astype(jnp.float32)
        conv = jnp.zeros((length, CW), jnp.float32)
        for tap in range(KW):
            conv = conv + conv_taps[tap].astype(jnp.float32) * padded[tap:tap + length]
        conv_out = (gate_b.astype(jnp.float32) * conv).astype(jnp.bfloat16)
        total_out = jnp.dot(attn, w_out_attn, preferred_element_type=jnp.float32) + jnp.dot(conv_out, w_out_conv, preferred_element_type=jnp.float32)
        return total_out.astype(jnp.bfloat16)
    return lax.map(one, tokens)
```

```python
import functools

import jax
import jax.numpy as jnp
from jax import lax
from jax.experimental import pallas as pl
from jax.experimental.pallas import tpu as pltpu
from jax.sharding import PartitionSpec as P

EPS = 1e-06
NEG = -1e30
OUT_SCALE = 0.8
HD = 128
HALF = HD // 2
PAIR = 2 * HD
TAIL = 8
F32 = jnp.float32
BF16 = jnp.bfloat16
MESH = pl.DeviceIdType.MESH


def kernel(
    n_sp,
    n_fs,
    tok_ref,
    norm_gain_ref,
    wq_ref,
    wk_ref,
    wv_ref,
    q_gain_ref,
    k_gain_ref,
    lam_ref,
    head_gain_ref,
    wb_ref,
    wc_ref,
    wi_ref,
    taps_ref,
    woa_ref,
    woc_ref,
    out_ref,
    tokens,
    stage,
    w_in,
    w_out,
    qkv,
    gate_b,
    heads,
    score,
    attn,
    attn_all,
    shaped,
    conv,
    conv_all,
    lams,
    w_send,
    w_recv,
    t_send,
    t_recv,
    ring_send,
    ring_recv,
    a_send,
    a_recv,
    kv_send,
    kv_recv,
    o_send,
    o_recv,
    c_send,
    c_recv,
    wo_send,
    wo_recv,
    one_send,
    one_recv,
):
    z, x, c = lax.axis_index("sp"), lax.axis_index("fs"), lax.axis_index("tp")
    own_seqs, rows, width = tok_ref.shape
    own_rows = own_seqs * rows
    block = 2 * rows
    keys = 2 * block
    part = wq_ref.shape[0]
    zpart = n_fs * part
    n_seq = own_seqs * n_fs
    half_ring = n_sp // 2
    xr, xl, xo = lax.rem(x + 1, n_fs), lax.rem(x + n_fs - 1, n_fs), lax.rem(x + 2, n_fs)
    zr, zl = lax.rem(z + 1, n_sp), lax.rem(z + n_sp - 1, n_sp)
    other = 1 - c
    me = n_fs * c + x

    def copy(src, dst, send, recv, **where):
        return pltpu.make_async_remote_copy(
            src_ref=src,
            dst_ref=dst,
            send_sem=send,
            recv_sem=recv,
            device_id=where,
            device_id_type=MESH,
        )

    barrier = pltpu.get_barrier_semaphore()
    near = [dict(fs=xr), dict(fs=xl), dict(fs=xo), dict(tp=other), dict(sp=zr), dict(sp=zl)]
    for where in near:
        pl.semaphore_signal(barrier, inc=1, device_id=where, device_id_type=MESH)

    sides = ((wq_ref, wk_ref), (wv_ref, wb_ref), (wc_ref, wi_ref), (woa_ref, woc_ref))
    for to in range(n_fs):
        lanes = slice(to * HD, (to + 1) * HD)
        for k, (left, right) in enumerate(sides):
            stage[to, k, :, 0:HD] = left[:, lanes]
            stage[to, k, :, HD:PAIR] = right[:, lanes]
    pl.semaphore_wait(barrier, len(near))

    here = pl.ds(pl.multiple_of(z * zpart + x * part, part), part)
    shard_copies = []
    for n, to in enumerate((xr, xl, xo)):
        shard_copies.append(
            copy(stage.at[to, 0:3], w_in.at[:, here, :], w_send.at[n, 0], w_recv.at[n, 0], fs=to)
        )
        shard_copies.append(
            copy(stage.at[to, 3], w_out.at[n_fs * c + to, here, :], w_send.at[n, 1], w_recv.at[n, 1], fs=to)
        )
    for sent in shard_copies:
        sent.start()
    w_in[:, here, :] = stage[x, 0:3]
    w_out[me, here, :] = stage[x, 3]

    step_rows = min(rows, 32)
    for s in range(own_seqs):
        for r in range(0, rows, step_rows):
            wide = tok_ref[s, r : r + step_rows, :].astype(F32)
            scale = lax.rsqrt(jnp.mean(wide * wide, axis=-1, keepdims=True) + EPS)
            at = pl.multiple_of(c * own_rows + s * rows + r, step_rows)
            tokens[x, pl.ds(at, step_rows), :] = (wide * scale * norm_gain_ref[...]).astype(BF16)

    class RowGather:
        def __init__(self, ref, size, send, recv):
            self.ref, self.size, self.send, self.recv = ref, size, send, recv

        def one(self, n, i, part_of, **where):
            first, length = ((0, self.size), (0, self.size // 2), (self.size // 2, self.size // 2))[part_of]
            ref = self.ref(i, first, length)
            return copy(ref, ref, self.send.at[n], self.recv.at[n], **where)

        def sent_as(self, n):
            i, part_of, where = (
                (x, 0, dict(fs=xr)),
                (x, 0, dict(fs=xl)),
                (xl, 1, dict(fs=xr)),
                (xr, 2, dict(fs=xl)),
                (x, 0, dict(tp=other)),
                (xl, 0, dict(tp=other)),
                (xr, 0, dict(tp=other)),
                (xo, 0, dict(tp=other)),
            )[n]
            return self.one(n, i, part_of, **where)

        def own(self):
            for n in (0, 1, 4):
                self.sent_as(n).start()

        def neighbours(self):
            self.one(0, xl, 0, fs=xr).wait_recv()
            self.sent_as(2).start()
            self.one(1, xr, 0, fs=xl).wait_recv()
            for n in (3, 5, 6):
                self.sent_as(n).start()

        def opposite(self):
            self.one(2, xo, 1, fs=xr).wait_recv()
            self.one(3, xo, 2, fs=xl).wait_recv()
            self.sent_as(7).start()

        def arrived(self, other_ref):
            mine, self.ref = self.ref, other_ref
            for n, i in ((4, x), (5, xl), (6, xr), (7, xo)):
                self.one(n, i, 0, tp=other).wait_recv()
            self.ref = mine

        def sent(self):
            for n in range(8):
                self.sent_as(n).wait_send()

    def token_ref(core):
        def ref(i, first, length):
            return tokens.at[i, pl.ds(pl.multiple_of(core * own_rows + first, length), length), :]

        return ref

    token_gather = RowGather(token_ref(c), own_rows, t_send, t_recv)
    token_gather.own()

    lane = lax.broadcasted_iota(jnp.int32, lam_ref.shape, 1)
    chosen = jnp.sum(jnp.where(lane == x, lam_ref[...], 0.0), axis=-1, keepdims=True)
    lams[c] = jnp.broadcast_to(chosen, lams.shape[1:])
    lam_copy = copy(lams.at[c], lams.at[c], one_send.at[0], one_recv.at[0], tp=other)
    lam_copy.start()

    def slice_ref(k, zb):
        at = pl.ds(pl.multiple_of(zb * zpart, zpart), zpart)
        return w_out.at[me, at, :] if k == 3 else w_in.at[k, at, :]

    def ring(way, step, k, ahead):
        if way == 0:
            zb, to = lax.rem(z - step - ahead + 2 * n_sp, n_sp), zr
        else:
            zb, to = lax.rem(z + step + ahead, n_sp), zl
        ref = slice_ref(k, zb)
        return copy(ref, ref, ring_send.at[way, step, k], ring_recv.at[way, step, k], sp=to)

    def active(way, step, k):
        return step < half_ring - 1 or (step == half_ring - 1 and (k < 2) == (way == 0))

    for n, source in enumerate((xl, xr, xo)):
        there = pl.ds(pl.multiple_of(z * zpart + source * part, part), part)
        copy(stage.at[x, 0:3], w_in.at[:, there, :], w_send.at[n, 0], w_recv.at[n, 0], fs=source).wait_recv()
        copy(stage.at[x, 3], w_out.at[me, there, :], w_send.at[n, 1], w_recv.at[n, 1], fs=source).wait_recv()
    for k in range(4):
        for way in range(2):
            ring(way, 0, k, 0).start()
    for step in range(half_ring):
        for k in range(4):
            for way in range(2):
                if active(way, step, k):
                    ring(way, step, k, 1).wait_recv()
                    if active(way, step + 1, k):
                        ring(way, step + 1, k, 0).start()
        if step == half_ring // 2 - 2:
            token_gather.neighbours()
        if step == half_ring // 2:
            token_gather.opposite()
    token_gather.arrived(token_ref(other))

    def w_out_ref(core):
        def ref(i, first, length):
            return w_out.at[n_fs * core + i, pl.ds(first, length), :]

        return ref

    w_out_gather = RowGather(w_out_ref(c), width, wo_send, wo_recv)

    lanes_x = pl.ds(pl.multiple_of(x * HD, HD), HD)
    low = lax.broadcasted_iota(jnp.int32, (2 * own_rows, HD), 1) < HALF

    def unit(raw, gain):
        wide = raw.astype(BF16).astype(F32)
        square = wide * wide
        first = jnp.sum(jnp.where(low, square, 0.0), axis=-1, keepdims=True)
        second = jnp.sum(jnp.where(low, 0.0, square), axis=-1, keepdims=True)
        scale = jnp.where(low, lax.rsqrt(first / HALF + EPS), lax.rsqrt(second / HALF + EPS))
        return wide * scale * gain

    @pl.loop(0, n_fs)
    def _(i):
        normed = tokens[i]
        both = jnp.dot(normed, w_in[0], preferred_element_type=F32)
        query = (unit(both[:, :HD], q_gain_ref[:, lanes_x]) * HALF**-0.5).astype(BF16)
        key = unit(both[:, HD:], k_gain_ref[:, lanes_x]).astype(BF16)
        both = jnp.dot(normed, w_in[1], preferred_element_type=F32).astype(BF16)
        gate_b[i] = both[:, HD:]
        for s in range(own_seqs):
            for core in range(2):
                src = slice(core * own_rows + s * rows, core * own_rows + (s + 1) * rows)
                dst = slice(core * rows, (core + 1) * rows)
                qkv[own_seqs * i + s, dst, 0:HD] = query[src]
                qkv[own_seqs * i + s, dst, HD:PAIR] = key[src]
                qkv[own_seqs * i + s, dst, PAIR:] = both[src, :HD]

    def owner(zb):
        return lax.rem(lax.rem(zb, 2) + zb // 2, 2)

    def own_block(i):
        return 2 * i + lax.rem(i + c, 2)

    def other_block(i):
        return 2 * i + lax.rem(i + other, 2)

    offsets = [n_seq // 2]
    for d in range(n_seq // 2 - 1, 0, -1):
        offsets += [d, n_seq - d]
    my_owner = owner(z)

    def qkv_copy(n, offset):
        s = lax.rem(z // 2 + offset, n_seq)
        return copy(qkv.at[s], heads.at[z], a_send.at[n], a_recv.at[z // 2], sp=2 * s + c, tp=my_owner)

    for n, offset in enumerate(offsets):
        qkv_copy(n, offset).start()
    last = len(offsets)
    home = (c == lax.rem(z, 2)) & (my_owner == c)
    away = (c != lax.rem(z, 2)) | (my_owner != c)

    @pl.when(away)
    def _():
        qkv_copy(last, 0).start()

    @pl.when(home)
    def _():
        heads[z] = qkv[z // 2]

    w_out_gather.own()

    @pl.loop(0, n_fs)
    def _(i):
        both = jnp.dot(tokens[i], w_in[2], preferred_element_type=F32).astype(BF16)
        both = both.astype(F32)
        product = (both[:, :HD] * both[:, HD:]).astype(BF16).astype(F32)
        for s in range(own_seqs):
            for core in range(2):
                src = slice(core * own_rows + s * rows, core * own_rows + (s + 1) * rows)
                shaped[own_seqs * i + s, TAIL + core * rows : TAIL + (core + 1) * rows, :] = product[src]

    tail_copy = copy(
        shaped.at[:, block : block + TAIL, :],
        shaped.at[:, 0:TAIL, :],
        one_send.at[1],
        one_recv.at[1],
        sp=zr,
    )
    tail_copy.start()
    tail_copy.wait_recv()

    @pl.when(z == 0)
    def _():
        shaped[:, 0:TAIL, :] = jnp.zeros((n_seq, TAIL, HD), F32)

    taps = [taps_ref[i : i + 1, lanes_x] for i in range(3)]

    @pl.loop(0, n_fs)
    def _(i):
        for s in range(own_seqs):
            seq = own_seqs * i + s
            total = taps[0] * shaped[seq, TAIL - 2 : TAIL - 2 + block, :]
            total = total + taps[1] * shaped[seq, TAIL - 1 : TAIL - 1 + block, :]
            total = total + taps[2] * shaped[seq, TAIL : TAIL + block, :]
            for core in range(2):
                gate = gate_b[i, core * own_rows + s * rows : core * own_rows + (s + 1) * rows, :]
                mixed = gate.astype(F32) * total[core * rows : (core + 1) * rows]
                conv[2 * i + core, s * rows : (s + 1) * rows, :] = mixed.astype(BF16)

    def conv_copy(n, to, core):
        return copy(conv.at[2 * to + core], conv_all.at[me], c_send.at[n], c_recv.at[me], fs=to, tp=core)

    conv_to = [(xo, c), (xo, other), (xr, c), (xr, other), (xl, c), (xl, other), (x, other)]
    for n, (to, core) in enumerate(conv_to):
        conv_copy(n, to, core).start()
    conv_all[me] = conv[2 * x + c]

    w_out_gather.neighbours()

    def kv_copy(i, zb):
        ref = heads.at[zb, :, HD:]
        return copy(ref, ref, kv_send.at[i], kv_recv.at[i], tp=other)

    for i in range(n_seq):
        zb = own_block(i)

        @pl.when((zb != z) | (c != lax.rem(z, 2)))
        def _():
            copy(qkv.at[0], heads.at[zb], a_send.at[0], a_recv.at[i], sp=zb, tp=c).wait_recv()

        kv_copy(i, zb).start()
    w_out_gather.opposite()
    lam_copy.wait_recv()
    for i in range(n_seq):
        kv_copy(i, other_block(i)).wait_recv()

    seq, mine = z // 2, lax.rem(z, 2)
    head = n_fs * mine + x
    seq_x, seq_row = seq // own_seqs, pl.ds(pl.multiple_of(lax.rem(seq, own_seqs) * rows, rows), rows)
    lane = lax.broadcasted_iota(jnp.int32, (block, HD), 1)
    key_at = lax.broadcasted_iota(jnp.int32, (2 * block, keys), 1)
    row_at = lax.rem(lax.broadcasted_iota(jnp.int32, (2 * block, keys), 0), block)

    def out_copy(i, zb, core):
        return copy(
            attn.at[i, core * rows : (core + 1) * rows, :],
            attn_all.at[head, seq_row, :],
            o_send.at[i, core],
            o_recv.at[head, lax.rem(seq, own_seqs)],
            fs=seq_x,
            sp=zb,
            tp=core,
        )

    def is_self(zb, core):
        return (seq_x == x) & (zb == z) & (c == core)

    def not_self(zb, core):
        return (seq_x != x) | (zb != z) | (c != core)

    def attend(i):
        zb = own_block(i)
        query = heads[zb, :, 0:HD].astype(F32)
        query = jnp.concatenate(
            [jnp.where(lane < HALF, query, 0.0), jnp.where(lane < HALF, 0.0, query)], axis=0
        ).astype(BF16)
        top = None
        for j in range(i + 1):
            key = heads[2 * j : 2 * j + 2, :, HD:PAIR].reshape(keys, HD)
            s = lax.dot_general(query, key, (((1,), (1,)), ((), ())), preferred_element_type=F32)
            if j == i:
                s = jnp.where(key_at <= row_at + block * lax.rem(i + c, 2), s, NEG)
            score[:, j * keys : (j + 1) * keys] = s
            best = functools.reduce(jnp.maximum, [s[:, n : n + HD] for n in range(0, keys, HD)] if keys >= HD else [s])
            top = best if top is None else jnp.maximum(top, best)
        top = jnp.max(top, axis=-1, keepdims=True)
        total, summed = None, None
        for j in range(i + 1):
            weight = jnp.exp(score[:, j * keys : (j + 1) * keys] - top)
            value = heads[2 * j : 2 * j + 2, :, PAIR:].reshape(keys, HD)
            add = jnp.dot(weight.astype(BF16), value, preferred_element_type=F32)
            w = sum(weight[:, n : n + HD] for n in range(0, keys, HD)) if keys >= HD else weight
            total = w if total is None else total + w
            summed = add if summed is None else summed + add
        maps = summed / jnp.sum(total, axis=-1, keepdims=True)
        differ = maps[:block] - lams[mine][0:1, :] * maps[block:]
        scale = lax.rsqrt(jnp.mean(differ * differ, axis=-1, keepdims=True) + EPS)
        attn[i] = (differ * scale * head_gain_ref[...] * OUT_SCALE).astype(BF16)
        for core in range(2):

            @pl.when(not_self(zb, core))
            def _():
                out_copy(i, zb, core).start()

            @pl.when(is_self(zb, core))
            def _():
                attn_all[head, seq_row, :] = attn[i, core * rows : (core + 1) * rows, :]

    @pl.loop(0, n_seq)
    def _(turn):
        now = lax.rem(z // 2 + turn, n_seq)
        for i in range(n_seq):

            @pl.when(now == i)
            def _():
                attend(i)

    w_out_gather.arrived(w_out_ref(other))
    for n, (to, core) in enumerate(conv_to):
        source = n_fs * core + to
        copy(conv.at[0], conv_all.at[source], c_send.at[n], c_recv.at[source], fs=to, tp=core).wait_recv()
    for h in range(2 * n_fs):
        for s in range(own_seqs):
            source_x, source_z = h % n_fs, 2 * (own_seqs * x + s) + h // n_fs

            @pl.when((source_x != x) | (source_z != z) | (my_owner != c))
            def _():
                copy(
                    attn.at[0, 0:rows, :],
                    attn_all.at[h, s * rows : (s + 1) * rows, :],
                    o_send.at[0, 0],
                    o_recv.at[h, s],
                    fs=source_x,
                    sp=source_z,
                    tp=my_owner,
                ).wait_recv()

    features = [jnp.concatenate([attn_all[h], conv_all[h]], axis=1) for h in range(2 * n_fs)]
    columns = min(width, 256)

    @pl.loop(0, width // columns)
    def _(n):
        at = pl.ds(pl.multiple_of(n * columns, columns), columns)
        total = None
        for h in range(2 * n_fs):
            add = lax.dot_general(
                features[h], w_out[h, at, :], (((1,), (1,)), ((), ())), preferred_element_type=F32
            )
            total = add if total is None else total + add
        for s in range(own_seqs):
            out_ref[s, :, at] = total[s * rows : (s + 1) * rows].astype(BF16)

    for sent in shard_copies:
        sent.wait_send()
    for step in range(half_ring):
        for k in range(4):
            for way in range(2):
                if active(way, step, k):
                    ring(way, step, k, 0).wait_send()
    token_gather.sent()
    w_out_gather.sent()
    lam_copy.wait_send()
    tail_copy.wait_send()
    for n, offset in enumerate(offsets):
        qkv_copy(n, offset).wait_send()

    @pl.when(away)
    def _():
        qkv_copy(last, 0).wait_send()

    for n, (to, core) in enumerate(conv_to):
        conv_copy(n, to, core).wait_send()
    for i in range(n_seq):
        zb = own_block(i)
        kv_copy(i, zb).wait_send()
        for core in range(2):

            @pl.when(not_self(zb, core))
            def _():
                out_copy(i, zb, core).wait_send()


def on_device(n_sp, n_fs, *args):
    tokens, norm_gain, wq, wk, wv, q_gain, k_gain, lam, head_gain, wb, wc, wi, taps, woa, woc = args
    own_seqs, rows, width = tokens.shape
    n_seq, block, n_head = own_seqs * n_fs, 2 * rows, 2 * n_fs
    assert n_sp == 2 * n_seq and n_fs == 4 and own_seqs == 2
    half_ring = n_sp // 2
    dma = pltpu.SemaphoreType.DMA
    vmem = pl.BlockSpec(memory_space=pltpu.VMEM)
    call = pl.pallas_call(
        functools.partial(kernel, n_sp, n_fs),
        out_shape=jax.ShapeDtypeStruct(tokens.shape, BF16),
        in_specs=[vmem] * 15,
        out_specs=vmem,
        scratch_shapes=[
            pltpu.VMEM((n_fs, 2 * own_seqs * rows, width), BF16),
            pltpu.VMEM((n_fs, 4, wq.shape[0], PAIR), BF16),
            pltpu.VMEM((3, width, PAIR), BF16),
            pltpu.VMEM((n_head, width, PAIR), BF16),
            pltpu.VMEM((n_seq, block, 3 * HD), BF16),
            pltpu.VMEM((n_fs, 2 * own_seqs * rows, HD), BF16),
            pltpu.VMEM((n_sp, block, 3 * HD), BF16),
            pltpu.VMEM((2 * block, n_sp * block), F32),
            pltpu.VMEM((n_seq, block, HD), BF16),
            pltpu.VMEM((n_head, own_seqs * rows, HD), BF16),
            pltpu.VMEM((n_seq, TAIL + block, HD), F32),
            pltpu.VMEM((n_head, own_seqs * rows, HD), BF16),
            pltpu.VMEM((n_head, own_seqs * rows, HD), BF16),
            pltpu.VMEM((2, 8, HD), F32),
            dma((3, 2)),
            dma((3, 2)),
            dma((8,)),
            dma((8,)),
            dma((2, half_ring, 4)),
            dma((2, half_ring, 4)),
            dma((n_seq,)),
            dma((n_seq,)),
            dma((n_seq,)),
            dma((n_seq,)),
            dma((n_seq, 2)),
            dma((n_head, own_seqs)),
            dma((n_head,)),
            dma((n_head,)),
            dma((8,)),
            dma((8,)),
            dma((2,)),
            dma((2,)),
        ],
        compiler_params=pltpu.CompilerParams(
            collective_id=0, has_side_effects=True, vmem_limit_bytes=56 * 1024 * 1024
        ),
    )
    row = lambda v: v.reshape(1, -1)
    return call(
        tokens, row(norm_gain), wq, wk, wv, row(q_gain), row(k_gain), row(lam), row(head_gain),
        wb, wc, wi, taps, woa.T, woc.T,
    )


def solution(mesh):
    placed = (
        P(("grp", "fs"), ("sp", "tp"), None),
        P(),
        P(("sp", "fs"), "tp"),
        P(("sp", "fs"), "tp"),
        P(("sp", "fs"), "tp"),
        P("tp"),
        P("tp"),
        P("tp"),
        P(),
        P(("sp", "fs"), "tp"),
        P(("sp", "fs"), "tp"),
        P(("sp", "fs"), "tp"),
        P(None, "tp"),
        P("tp", ("sp", "fs")),
        P("tp", ("sp", "fs")),
    )
    return jax.shard_map(
        functools.partial(on_device, mesh.shape["sp"], mesh.shape["fs"]),
        mesh=mesh,
        in_specs=placed,
        out_specs=P(("grp", "fs"), ("sp", "tp"), None),
        check_vma=False,
    )
```

```python
import functools

import jax
import jax.numpy as jnp
from jax import lax
from jax.experimental import pallas as pl
from jax.experimental.pallas import tpu as pltpu
from jax.sharding import PartitionSpec as P

EPS = 1e-06
NEG = -1e30
OUT_SCALE = 0.8
HD = 128
HALF = HD // 2
PAIR = 2 * HD
TAIL = 8
F32 = jnp.float32
BF16 = jnp.bfloat16
MESH = pl.DeviceIdType.MESH


def kernel(
    n_grp,
    n_sp,
    n_fs,
    tok_ref,
    norm_gain_ref,
    wq_ref,
    wk_ref,
    wv_ref,
    q_gain_ref,
    k_gain_ref,
    lam_ref,
    head_gain_ref,
    wb_ref,
    wc_ref,
    wi_ref,
    taps_ref,
    woa_ref,
    woc_ref,
    out_ref,
    tokens,
    stage,
    wall,
    qkv,
    gate_b,
    heads,
    score,
    attn,
    attn_all,
    shaped,
    conv,
    conv_all,
    lams,
    w_send,
    w_recv,
    t_send,
    t_recv,
    ring_send,
    ring_recv,
    pair_send,
    pair_recv,
    ready,
    a_send,
    a_recv,
    kv_send,
    kv_recv,
    o_send,
    o_recv,
    c_send,
    c_recv,
    wo_send,
    wo_recv,
    one_send,
    one_recv,
):
    g = lax.axis_index("grp")
    z, x, c = lax.axis_index("sp"), lax.axis_index("fs"), lax.axis_index("tp")
    own_seqs, rows, width = tok_ref.shape
    own_rows = own_seqs * rows
    block = 2 * rows
    keys = 2 * block
    part = wq_ref.shape[0]
    zpart = n_fs * part
    n_seq = own_seqs * n_fs
    half_ring = n_sp // 2
    xr, xl, xo = lax.rem(x + 1, n_fs), lax.rem(x + n_fs - 1, n_fs), lax.rem(x + 2, n_fs)
    zr, zl = lax.rem(z + 1, n_sp), lax.rem(z + n_sp - 1, n_sp)
    other = 1 - c
    me = n_fs * c + x
    odd = lax.rem(g, 2)
    pair = g + 1 - 2 * odd
    out_at = 3

    def copy(src, dst, send, recv, **where):
        return pltpu.make_async_remote_copy(
            src_ref=src,
            dst_ref=dst,
            send_sem=send,
            recv_sem=recv,
            device_id=where,
            device_id_type=MESH,
        )

    barrier = pltpu.get_barrier_semaphore()
    near = [dict(fs=xr), dict(fs=xl), dict(fs=xo), dict(tp=other), dict(sp=zl), dict(grp=pair)]
    for where in near:
        pl.semaphore_signal(barrier, inc=1, device_id=where, device_id_type=MESH)

    sides = ((wq_ref, wk_ref), (wv_ref, wb_ref), (wc_ref, wi_ref), (woa_ref, woc_ref))
    for to in range(n_fs):
        lanes = slice(to * HD, (to + 1) * HD)
        for k, (left, right) in enumerate(sides):
            stage[to, k, :, 0:HD] = left[:, lanes]
            stage[to, k, :, HD:PAIR] = right[:, lanes]
    pl.semaphore_wait(barrier, len(near))

    pl.semaphore_signal(ready, inc=1, device_id=dict(sp=zr), device_id_type=MESH)

    def chunk_at(k, to):
        return out_at + n_fs * c + to if k == 3 else k

    def shard_copy(k, n, to, source):
        at = pl.ds(pl.multiple_of(z * zpart + source * part, part), part)
        return copy(stage.at[to, k], wall.at[chunk_at(k, to), at, :], w_send.at[n, k], w_recv.at[n, k], fs=to)

    for k in range(4):
        for n, to in ((2, xo), (0, xr), (1, xl)):
            shard_copy(k, n, to, x).start()
    here = pl.ds(pl.multiple_of(z * zpart + x * part, part), part)
    wall[0:3, here, :] = stage[x, 0:3]
    wall[out_at + me, here, :] = stage[x, 3]

    step_rows = min(rows, 32)
    for s in range(own_seqs):
        for r in range(0, rows, step_rows):
            wide = tok_ref[s, r : r + step_rows, :].astype(F32)
            scale = lax.rsqrt(jnp.mean(wide * wide, axis=-1, keepdims=True) + EPS)
            at = pl.multiple_of(c * own_rows + s * rows + r, step_rows)
            tokens[x, pl.ds(at, step_rows), :] = (wide * scale * norm_gain_ref[...]).astype(BF16)

    class RowGather:
        def __init__(self, ref, size, send, recv, j):
            self.ref, self.size, self.send, self.recv, self.j = ref, size, send, recv, j

        def one(self, n, i, part_of, **where):
            first, length = ((0, self.size), (0, self.size // 2), (self.size // 2, self.size // 2))[part_of]
            ref = self.ref(i, first, length)
            return copy(ref, ref, self.send.at[self.j, n], self.recv.at[self.j, n], **where)

        def sent_as(self, n):
            i, part_of, where = (
                (x, 0, dict(fs=xr)),
                (x, 0, dict(fs=xl)),
                (xl, 1, dict(fs=xr)),
                (xr, 2, dict(fs=xl)),
                (x, 0, dict(tp=other)),
                (xl, 0, dict(tp=other)),
                (xr, 0, dict(tp=other)),
                (xo, 0, dict(tp=other)),
            )[n]
            return self.one(n, i, part_of, **where)

        def own(self):
            for n in (0, 1, 4):
                self.sent_as(n).start()

        def neighbours(self):
            self.one(0, xl, 0, fs=xr).wait_recv()
            self.sent_as(2).start()
            self.one(1, xr, 0, fs=xl).wait_recv()
            for n in (3, 5, 6):
                self.sent_as(n).start()

        def opposite(self):
            self.one(2, xo, 1, fs=xr).wait_recv()
            self.one(3, xo, 2, fs=xl).wait_recv()
            self.sent_as(7).start()

        def arrived(self, other_ref):
            mine, self.ref = self.ref, other_ref
            for n, i in ((4, x), (5, xl), (6, xr), (7, xo)):
                self.one(n, i, 0, tp=other).wait_recv()
            self.ref = mine

        def sent(self):
            for n in range(8):
                self.sent_as(n).wait_send()

    def token_ref(core):
        def ref(i, first, length):
            return tokens.at[i, pl.ds(pl.multiple_of(core * own_rows + first, length), length), :]

        return ref

    token_gather = RowGather(token_ref(c), own_rows, t_send, t_recv, 0)
    token_gather.own()

    lane = lax.broadcasted_iota(jnp.int32, lam_ref.shape, 1)
    chosen = jnp.sum(jnp.where(lane == x, lam_ref[...], 0.0), axis=-1, keepdims=True)
    lams[c] = jnp.broadcast_to(chosen, lams.shape[1:])
    lam_copy = copy(lams.at[c], lams.at[c], one_send.at[0], one_recv.at[0], tp=other)
    lam_copy.start()

    slots = (0, 1, 2 + odd * (1 + me))
    from_pair = 2 + (1 - odd) * (1 + me)

    def slice_ref(at, zb):
        return wall.at[at, pl.ds(pl.multiple_of(zb * zpart, zpart), zpart), :]

    def ring_block(way, step):
        return lax.rem(z - step + 2 * n_sp, n_sp) if way == 0 else lax.rem(z + step, n_sp)

    def ring(way, step, k, ahead):
        ref = slice_ref(slots[k], ring_block(way, step + ahead))
        to = zr if way == 0 else zl
        return copy(ref, ref, ring_send.at[way, step, k], ring_recv.at[way, step, k], sp=to)

    def pair_copy(way, step, at):
        ref = slice_ref(at, ring_block(way, step + 1))
        return copy(ref, ref, pair_send.at[way, step], pair_recv.at[way, step], grp=pair)

    def active(way, step, k):
        return step < half_ring - 1 or (step == half_ring - 1 and (k == 0) == (way == 0))

    hops = [(way, step) for step in range(half_ring) for way in range(2) if active(way, step, 2)]

    for k in range(4):
        for n, source in ((2, xo), (0, xl), (1, xr)):
            shard_copy(k, n, x, source).wait_recv()
        for slot, its in enumerate(((0,), (1,), (2, 3))):
            if k == its[-1]:
                ring(0, 0, slot, 0).start()
    pl.semaphore_wait(ready, 1)
    for k in range(3):
        ring(1, 0, k, 0).start()
    for step in range(half_ring):
        for k in range(3):
            for way in range(2):
                if active(way, step, k):
                    ring(way, step, k, 1).wait_recv()
                    if active(way, step + 1, k):
                        ring(way, step + 1, k, 0).start()
                    if k == 2:
                        pair_copy(way, step, slots[2]).start()
        if step == 2:
            token_gather.neighbours()
        if step == 4:
            token_gather.opposite()
    token_gather.arrived(token_ref(other))

    pieces = wo_send.shape[0]
    piece = width // pieces

    def w_out_ref(core, j):
        def ref(i, first, length):
            return wall.at[out_at + n_fs * core + i, pl.ds(j * piece + first, length), :]

        return ref

    w_out_gathers = [RowGather(w_out_ref(c, j), piece, wo_send, wo_recv, j) for j in range(pieces)]

    lanes_x = pl.ds(pl.multiple_of(x * HD, HD), HD)
    low = lax.broadcasted_iota(jnp.int32, (2 * own_rows, HD), 1) < HALF

    def unit(raw, gain):
        wide = raw.astype(BF16).astype(F32)
        square = wide * wide
        first = jnp.sum(jnp.where(low, square, 0.0), axis=-1, keepdims=True)
        second = jnp.sum(jnp.where(low, 0.0, square), axis=-1, keepdims=True)
        scale = jnp.where(low, lax.rsqrt(first / HALF + EPS), lax.rsqrt(second / HALF + EPS))
        return wide * scale * gain

    @pl.loop(0, n_fs)
    def _(i):
        normed = tokens[i]
        both = jnp.dot(normed, wall[0], preferred_element_type=F32)
        query = (unit(both[:, :HD], q_gain_ref[:, lanes_x]) * HALF**-0.5).astype(BF16)
        key = unit(both[:, HD:], k_gain_ref[:, lanes_x]).astype(BF16)
        both = jnp.dot(normed, wall[1], preferred_element_type=F32).astype(BF16)
        gate_b[i] = both[:, HD:]
        for s in range(own_seqs):
            for core in range(2):
                src = slice(core * own_rows + s * rows, core * own_rows + (s + 1) * rows)
                dst = slice(core * rows, (core + 1) * rows)
                qkv[own_seqs * i + s, dst, 0:HD] = query[src]
                qkv[own_seqs * i + s, dst, HD:PAIR] = key[src]
                qkv[own_seqs * i + s, dst, PAIR:] = both[src, :HD]

    def owner(zb):
        return lax.rem(lax.rem(zb, 2) + zb // 2, 2)

    def own_block(i):
        return 2 * i + lax.rem(i + c, 2)

    def other_block(i):
        return 2 * i + lax.rem(i + other, 2)

    offsets = [n_seq // 2]
    for d in range(n_seq // 2 - 1, 0, -1):
        offsets += [d, n_seq - d]
    my_owner = owner(z)

    def qkv_copy(n, offset):
        s = lax.rem(z // 2 + offset, n_seq)
        return copy(qkv.at[s], heads.at[z], a_send.at[n], a_recv.at[z // 2], sp=2 * s + c, tp=my_owner)

    for n, offset in enumerate(offsets):
        qkv_copy(n, offset).start()
    last = len(offsets)
    home = (c == lax.rem(z, 2)) & (my_owner == c)
    away = (c != lax.rem(z, 2)) | (my_owner != c)

    @pl.when(away)
    def _():
        qkv_copy(last, 0).start()

    @pl.when(home)
    def _():
        heads[z] = qkv[z // 2]

    for way, step in hops:
        pair_copy(way, step, from_pair).wait_recv()
    for gather in w_out_gathers:
        gather.own()

    @pl.loop(0, n_fs)
    def _(i):
        both = jnp.dot(tokens[i], wall[2], preferred_element_type=F32).astype(BF16)
        both = both.astype(F32)
        product = (both[:, :HD] * both[:, HD:]).astype(BF16).astype(F32)
        for s in range(own_seqs):
            for core in range(2):
                src = slice(core * own_rows + s * rows, core * own_rows + (s + 1) * rows)
                shaped[own_seqs * i + s, TAIL + core * rows : TAIL + (core + 1) * rows, :] = product[src]

    tail_copy = copy(
        shaped.at[:, block : block + TAIL, :],
        shaped.at[:, 0:TAIL, :],
        one_send.at[1],
        one_recv.at[1],
        sp=zr,
    )
    tail_copy.start()
    for gather in w_out_gathers:
        gather.neighbours()

    def kv_copy(i, zb):
        ref = heads.at[zb, :, HD:]
        return copy(ref, ref, kv_send.at[i], kv_recv.at[i], tp=other)

    for i in range(n_seq):
        zb = own_block(i)

        @pl.when((zb != z) | (c != lax.rem(z, 2)))
        def _():
            copy(qkv.at[0], heads.at[zb], a_send.at[0], a_recv.at[i], sp=zb, tp=c).wait_recv()

        kv_copy(i, zb).start()
    lam_copy.wait_recv()
    for i in range(n_seq):
        kv_copy(i, other_block(i)).wait_recv()

    seq, mine = z // 2, lax.rem(z, 2)
    head = n_fs * mine + x
    seq_x, seq_row = seq // own_seqs, pl.ds(pl.multiple_of(lax.rem(seq, own_seqs) * rows, rows), rows)
    lane = lax.broadcasted_iota(jnp.int32, (block, HD), 1)
    key_at = lax.broadcasted_iota(jnp.int32, (2 * block, keys), 1)
    row_at = lax.rem(lax.broadcasted_iota(jnp.int32, (2 * block, keys), 0), block)

    def out_copy(i, zb, core):
        return copy(
            attn.at[i, core * rows : (core + 1) * rows, :],
            attn_all.at[head, seq_row, :],
            o_send.at[i, core],
            o_recv.at[head, lax.rem(seq, own_seqs)],
            fs=seq_x,
            sp=zb,
            tp=core,
        )

    def is_self(zb, core):
        return (seq_x == x) & (zb == z) & (c == core)

    def not_self(zb, core):
        return (seq_x != x) | (zb != z) | (c != core)

    def attend(i):
        zb = own_block(i)
        query = heads[zb, :, 0:HD].astype(F32)
        query = jnp.concatenate(
            [jnp.where(lane < HALF, query, 0.0), jnp.where(lane < HALF, 0.0, query)], axis=0
        ).astype(BF16)
        top = None
        for j in range(i + 1):
            key = heads[2 * j : 2 * j + 2, :, HD:PAIR].reshape(keys, HD)
            s = lax.dot_general(query, key, (((1,), (1,)), ((), ())), preferred_element_type=F32)
            if j == i:
                s = jnp.where(key_at <= row_at + block * lax.rem(i + c, 2), s, NEG)
            score[:, j * keys : (j + 1) * keys] = s
            best = functools.reduce(jnp.maximum, [s[:, n : n + HD] for n in range(0, keys, HD)] if keys >= HD else [s])
            top = best if top is None else jnp.maximum(top, best)
        top = jnp.max(top, axis=-1, keepdims=True)
        total, summed = None, None
        for j in range(i + 1):
            weight = jnp.exp(score[:, j * keys : (j + 1) * keys] - top)
            value = heads[2 * j : 2 * j + 2, :, PAIR:].reshape(keys, HD)
            add = jnp.dot(weight.astype(BF16), value, preferred_element_type=F32)
            w = sum(weight[:, n : n + HD] for n in range(0, keys, HD)) if keys >= HD else weight
            total = w if total is None else total + w
            summed = add if summed is None else summed + add
        maps = summed / jnp.sum(total, axis=-1, keepdims=True)
        differ = maps[:block] - lams[mine][0:1, :] * maps[block:]
        scale = lax.rsqrt(jnp.mean(differ * differ, axis=-1, keepdims=True) + EPS)
        attn[i] = (differ * scale * head_gain_ref[...] * OUT_SCALE).astype(BF16)
        for core in range(2):

            @pl.when(not_self(zb, core))
            def _():
                out_copy(i, zb, core).start()

            @pl.when(is_self(zb, core))
            def _():
                attn_all[head, seq_row, :] = attn[i, core * rows : (core + 1) * rows, :]

    @pl.loop(0, n_seq)
    def _(turn):
        now = lax.rem(z // 2 + turn, n_seq)
        for i in range(n_seq):

            @pl.when(now == i)
            def _():
                attend(i)

    for gather in w_out_gathers:
        gather.opposite()
    tail_copy.wait_recv()

    @pl.when(z == 0)
    def _():
        shaped[:, 0:TAIL, :] = jnp.zeros((n_seq, TAIL, HD), F32)

    taps = [taps_ref[i : i + 1, lanes_x] for i in range(3)]

    @pl.loop(0, n_fs)
    def _(i):
        for s in range(own_seqs):
            seq = own_seqs * i + s
            total = taps[0] * shaped[seq, TAIL - 2 : TAIL - 2 + block, :]
            total = total + taps[1] * shaped[seq, TAIL - 1 : TAIL - 1 + block, :]
            total = total + taps[2] * shaped[seq, TAIL : TAIL + block, :]
            for core in range(2):
                gate = gate_b[i, core * own_rows + s * rows : core * own_rows + (s + 1) * rows, :]
                mixed = gate.astype(F32) * total[core * rows : (core + 1) * rows]
                conv[2 * i + core, s * rows : (s + 1) * rows, :] = mixed.astype(BF16)

    def conv_copy(n, to, core):
        return copy(conv.at[2 * to + core], conv_all.at[me], c_send.at[n], c_recv.at[me], fs=to, tp=core)

    conv_to = [(xo, c), (xo, other), (xr, c), (xr, other), (xl, c), (xl, other), (x, other)]
    for n, (to, core) in enumerate(conv_to):
        conv_copy(n, to, core).start()
    conv_all[me] = conv[2 * x + c]


    for j, gather in enumerate(w_out_gathers):
        gather.arrived(w_out_ref(other, j))
    for n, (to, core) in enumerate(conv_to):
        source = n_fs * core + to
        copy(conv.at[0], conv_all.at[source], c_send.at[n], c_recv.at[source], fs=to, tp=core).wait_recv()
    for h in range(2 * n_fs):
        for s in range(own_seqs):
            source_x, source_z = h % n_fs, 2 * (own_seqs * x + s) + h // n_fs

            @pl.when((source_x != x) | (source_z != z) | (my_owner != c))
            def _():
                copy(
                    attn.at[0, 0:rows, :],
                    attn_all.at[h, s * rows : (s + 1) * rows, :],
                    o_send.at[0, 0],
                    o_recv.at[h, s],
                    fs=source_x,
                    sp=source_z,
                    tp=my_owner,
                ).wait_recv()

    features = [jnp.concatenate([attn_all[h], conv_all[h]], axis=1) for h in range(2 * n_fs)]
    columns = min(width, 256)

    @pl.loop(0, width // columns)
    def _(n):
        at = pl.ds(pl.multiple_of(n * columns, columns), columns)
        total = None
        for h in range(2 * n_fs):
            add = lax.dot_general(
                features[h], wall[out_at + h, at, :], (((1,), (1,)), ((), ())), preferred_element_type=F32
            )
            total = add if total is None else total + add
        for s in range(own_seqs):
            out_ref[s, :, at] = total[s * rows : (s + 1) * rows].astype(BF16)

    for k in range(4):
        for n, to in enumerate((xr, xl, xo)):
            shard_copy(k, n, to, x).wait_send()
    for way, step in hops:
        pair_copy(way, step, slots[2]).wait_send()
    for step in range(half_ring):
        for k in range(3):
            for way in range(2):
                if active(way, step, k):
                    ring(way, step, k, 0).wait_send()
    token_gather.sent()
    for gather in w_out_gathers:
        gather.sent()
    lam_copy.wait_send()
    tail_copy.wait_send()
    for n, offset in enumerate(offsets):
        qkv_copy(n, offset).wait_send()

    @pl.when(away)
    def _():
        qkv_copy(last, 0).wait_send()

    for n, (to, core) in enumerate(conv_to):
        conv_copy(n, to, core).wait_send()
    for i in range(n_seq):
        zb = own_block(i)
        kv_copy(i, zb).wait_send()
        for core in range(2):

            @pl.when(not_self(zb, core))
            def _():
                out_copy(i, zb, core).wait_send()


def on_device(n_grp, n_sp, n_fs, *args):
    tokens, norm_gain, wq, wk, wv, q_gain, k_gain, lam, head_gain, wb, wc, wi, taps, woa, woc = args
    own_seqs, rows, width = tokens.shape
    n_seq, block, n_head = own_seqs * n_fs, 2 * rows, 2 * n_fs
    assert n_grp % 2 == 0 and n_sp == 2 * n_seq and n_fs == 4 and own_seqs == 2
    half_ring = n_sp // 2
    dma = pltpu.SemaphoreType.DMA
    vmem = pl.BlockSpec(memory_space=pltpu.VMEM)
    call = pl.pallas_call(
        functools.partial(kernel, n_grp, n_sp, n_fs),
        out_shape=jax.ShapeDtypeStruct(tokens.shape, BF16),
        in_specs=[vmem] * 15,
        out_specs=vmem,
        scratch_shapes=[
            pltpu.VMEM((n_fs, 2 * own_seqs * rows, width), BF16),
            pltpu.VMEM((n_fs, 4, wq.shape[0], PAIR), BF16),
            pltpu.VMEM((3 + n_head, width, PAIR), BF16),
            pltpu.VMEM((n_seq, block, 3 * HD), BF16),
            pltpu.VMEM((n_fs, 2 * own_seqs * rows, HD), BF16),
            pltpu.VMEM((n_sp, block, 3 * HD), BF16),
            pltpu.VMEM((2 * block, n_sp * block), F32),
            pltpu.VMEM((n_seq, block, HD), BF16),
            pltpu.VMEM((n_head, own_seqs * rows, HD), BF16),
            pltpu.VMEM((n_seq, TAIL + block, HD), F32),
            pltpu.VMEM((n_head, own_seqs * rows, HD), BF16),
            pltpu.VMEM((n_head, own_seqs * rows, HD), BF16),
            pltpu.VMEM((2, 8, HD), F32),
            dma((3, 4)),
            dma((3, 4)),
            dma((1, 8)),
            dma((1, 8)),
            dma((2, half_ring, 3)),
            dma((2, half_ring, 3)),
            dma((2, half_ring)),
            dma((2, half_ring)),
            pltpu.SemaphoreType.REGULAR,
            dma((n_seq,)),
            dma((n_seq,)),
            dma((n_seq,)),
            dma((n_seq,)),
            dma((n_seq, 2)),
            dma((n_head, own_seqs)),
            dma((n_head,)),
            dma((n_head,)),
            dma((4, 8)),
            dma((4, 8)),
            dma((2,)),
            dma((2,)),
        ],
        compiler_params=pltpu.CompilerParams(
            collective_id=0, has_side_effects=True, vmem_limit_bytes=56 * 1024 * 1024
        ),
    )
    row = lambda v: v.reshape(1, -1)
    return call(
        tokens, row(norm_gain), wq, wk, wv, row(q_gain), row(k_gain), row(lam), row(head_gain),
        wb, wc, wi, taps, woa.T, woc.T,
    )


def solution(mesh):
    placed = (
        P(("grp", "fs"), ("sp", "tp"), None),
        P(),
        P(("sp", "fs"), "tp"),
        P(("sp", "fs"), "tp"),
        P(("sp", "fs"), "tp"),
        P("tp"),
        P("tp"),
        P("tp"),
        P(),
        P(("sp", "fs"), "tp"),
        P(("sp", "fs"), "tp"),
        P(("sp", "fs"), "tp"),
        P(None, "tp"),
        P("tp", ("sp", "fs")),
        P("tp", ("sp", "fs")),
    )
    return jax.shard_map(
        functools.partial(on_device, mesh.shape["grp"], mesh.shape["sp"], mesh.shape["fs"]),
        mesh=mesh,
        in_specs=placed,
        out_specs=P(("grp", "fs"), ("sp", "tp"), None),
        check_vma=False,
    )
```

```python
import functools

import jax
import jax.numpy as jnp
from jax import lax
from jax.experimental import pallas as pl
from jax.experimental.pallas import tpu as pltpu
from jax.sharding import PartitionSpec as P

EPS = 1e-06
NEG = -1e30
OUT_SCALE = 0.8
HD = 128
HALF = HD // 2
PAIR = 2 * HD
TAIL = 8
F32 = jnp.float32
BF16 = jnp.bfloat16
MESH = pl.DeviceIdType.MESH


def kernel(
    n_grp,
    n_sp,
    n_fs,
    *refs,
):
    (tok_ref, norm_gain_ref, wq_ref, wk_ref, wv_ref, q_gain_ref, k_gain_ref, lam_ref, head_gain_ref, wb_ref, wc_ref, wi_ref, taps_ref, woa_ref, woc_ref) = refs[16:31]
    (
    out_ref,
    tokens,
    stage,
    wall,
    partial,
    qkv,
    gate_b,
    heads,
    score,
    attn,
    attn_all,
    shaped,
    conv,
    conv_all,
    lams,
    mixed,
    w_send,
    w_recv,
    t_send,
    t_recv,
    ring_send,
    ring_recv,
    pair_send,
    pair_recv,
    ready,
    a_send,
    a_recv,
    kv_send,
    kv_recv,
    o_send,
    o_recv,
    c_send,
    c_recv,
    wo_send,
    wo_recv,
    one_send,
    one_recv,
    load_sem,
    ) = (refs[15], *refs[31:])
    loads = [pltpu.make_async_copy(refs[n], refs[16 + n], load_sem.at[n]) for n in range(15)]
    for n in (2, 3, 4, 9, 10, 11, 13, 14, 0, 1, 5, 6, 7, 8, 12):
        loads[n].start()
    g = lax.axis_index("grp")
    z, x, c = lax.axis_index("sp"), lax.axis_index("fs"), lax.axis_index("tp")
    own_seqs, rows, width = tok_ref.shape
    own_rows = own_seqs * rows
    block = 2 * rows
    keys = 2 * block
    part = wq_ref.shape[0]
    zpart = n_fs * part
    n_seq = own_seqs * n_fs
    half_ring = n_sp // 2
    xr, xl, xo = lax.rem(x + 1, n_fs), lax.rem(x + n_fs - 1, n_fs), lax.rem(x + 2, n_fs)
    zr, zl = lax.rem(z + 1, n_sp), lax.rem(z + n_sp - 1, n_sp)
    other = 1 - c
    me = n_fs * c + x
    odd = lax.rem(g, 2)
    pair = g + 1 - 2 * odd
    out_at = 3

    def copy(src, dst, send, recv, **where):
        return pltpu.make_async_remote_copy(
            src_ref=src,
            dst_ref=dst,
            send_sem=send,
            recv_sem=recv,
            device_id=where,
            device_id_type=MESH,
        )

    barrier = pltpu.get_barrier_semaphore()
    near = [dict(fs=xr), dict(fs=xl), dict(fs=xo), dict(tp=other), dict(sp=zl), dict(grp=pair)]
    for where in near:
        pl.semaphore_signal(barrier, inc=1, device_id=where, device_id_type=MESH)

    for n in range(15):
        loads[n].wait()

    sides = ((wq_ref, wk_ref), (wv_ref, wb_ref), (wc_ref, wi_ref), (woa_ref, woc_ref))
    for to in range(n_fs):
        lanes = slice(to * HD, (to + 1) * HD)
        for k, (left, right) in enumerate(sides):
            stage[to, k, :, 0:HD] = left[:, lanes]
            stage[to, k, :, HD:PAIR] = right[:, lanes]
    pl.semaphore_wait(barrier, len(near))

    pl.semaphore_signal(ready, inc=1, device_id=dict(sp=zr), device_id_type=MESH)

    def chunk_at(k, to):
        return out_at + n_fs * c + to if k == 3 else k

    def shard_copy(k, n, to, source):
        at = pl.ds(pl.multiple_of(z * zpart + source * part, part), part)
        return copy(stage.at[to, k], wall.at[chunk_at(k, to), at, :], w_send.at[n, k], w_recv.at[n, k], fs=to)

    for k in range(4):
        for n, to in ((2, xo), (0, xr), (1, xl)):
            shard_copy(k, n, to, x).start()
    here = pl.ds(pl.multiple_of(z * zpart + x * part, part), part)
    wall[0:3, here, :] = stage[x, 0:3]
    wall[out_at + me, here, :] = stage[x, 3]

    step_rows = min(rows, 32)
    for s in range(own_seqs):
        for r in range(0, rows, step_rows):
            wide = tok_ref[s, r : r + step_rows, :].astype(F32)
            scale = lax.rsqrt(jnp.mean(wide * wide, axis=-1, keepdims=True) + EPS)
            at = pl.multiple_of(c * own_rows + s * rows + r, step_rows)
            tokens[x, pl.ds(at, step_rows), :] = (wide * scale * norm_gain_ref[...]).astype(BF16)

    class RowGather:
        def __init__(self, ref, size, send, recv, j):
            self.ref, self.size, self.send, self.recv, self.j = ref, size, send, recv, j

        def one(self, n, i, part_of, **where):
            first, length = ((0, self.size), (0, self.size // 2), (self.size // 2, self.size // 2))[part_of]
            ref = self.ref(i, first, length)
            return copy(ref, ref, self.send.at[self.j, n], self.recv.at[self.j, n], **where)

        def sent_as(self, n):
            i, part_of, where = (
                (x, 0, dict(fs=xr)),
                (x, 0, dict(fs=xl)),
                (xl, 1, dict(fs=xr)),
                (xr, 2, dict(fs=xl)),
                (x, 0, dict(tp=other)),
                (xl, 0, dict(tp=other)),
                (xr, 0, dict(tp=other)),
                (xo, 0, dict(tp=other)),
            )[n]
            return self.one(n, i, part_of, **where)

        def own(self):
            for n in (0, 1, 4):
                self.sent_as(n).start()

        def neighbours(self):
            self.one(0, xl, 0, fs=xr).wait_recv()
            self.sent_as(2).start()
            self.one(1, xr, 0, fs=xl).wait_recv()
            for n in (3, 5, 6):
                self.sent_as(n).start()

        def opposite(self):
            self.one(2, xo, 1, fs=xr).wait_recv()
            self.one(3, xo, 2, fs=xl).wait_recv()
            self.sent_as(7).start()

        def arrived(self, other_ref):
            mine, self.ref = self.ref, other_ref
            for n, i in ((4, x), (5, xl), (6, xr), (7, xo)):
                self.one(n, i, 0, tp=other).wait_recv()
            self.ref = mine

        def sent(self):
            for n in range(8):
                self.sent_as(n).wait_send()

    def token_ref(core):
        def ref(i, first, length):
            return tokens.at[i, pl.ds(pl.multiple_of(core * own_rows + first, length), length), :]

        return ref

    token_gather = RowGather(token_ref(c), own_rows, t_send, t_recv, 0)
    token_gather.own()

    lane = lax.broadcasted_iota(jnp.int32, lam_ref.shape, 1)
    chosen = jnp.sum(jnp.where(lane == x, lam_ref[...], 0.0), axis=-1, keepdims=True)
    lams[c] = jnp.broadcast_to(chosen, lams.shape[1:])
    lam_copy = copy(lams.at[c], lams.at[c], one_send.at[0], one_recv.at[0], tp=other)
    lam_copy.start()

    def slice_ref(k, zb, side):
        first = zb * zpart
        if k == 3:
            first, length = first + side * (zpart // 2), zpart // 2
        else:
            length = zpart
        at = pl.ds(pl.multiple_of(first, length), length)
        if k == 2:
            return wall.at[2 + side * (1 + me), at, :]
        return wall.at[(0, 1, 2, 1)[k], at, (slice(0, PAIR), slice(0, HD), None, slice(HD, PAIR))[k]]

    def ring_block(way, step):
        return lax.rem(z - step + 2 * n_sp, n_sp) if way == 0 else lax.rem(z + step, n_sp)

    def ring(way, step, k, ahead):
        ref = slice_ref(k, ring_block(way, step + ahead), odd)
        to = zr if way == 0 else zl
        return copy(ref, ref, ring_send.at[way, step, k], ring_recv.at[way, step, k], sp=to)

    def pair_copy(way, step, k, side):
        ref = slice_ref(k, ring_block(way, step + 1), side)
        return copy(ref, ref, pair_send.at[k - 2, way, step], pair_recv.at[k - 2, way, step], grp=pair)

    def active(way, step, k):
        return step < half_ring - 1 or (step == half_ring - 1 and (k in (0, 3)) == (way == 0))

    hops = [(way, step, k) for step in range(half_ring) for k in (2, 3) for way in range(2) if active(way, step, k)]

    @pl.when(z != 0)
    def _():
        pl.semaphore_wait(ready, 1)

    for k in range(4):
        for n, source in ((2, xo), (0, xl), (1, xr)):
            shard_copy(k, n, x, source).wait_recv()
        for slot, its in enumerate((0, 1, 3, 1)):
            if k == its:
                ring(0, 0, slot, 0).start()

                @pl.when(z != 0)
                def _():
                    ring(1, 0, slot, 0).start()

    @pl.when(z == 0)
    def _():
        pl.semaphore_wait(ready, 1)
        for k in range(4):
            ring(1, 0, k, 0).start()

    def project(i, blocks, first=False):
        for k in range(2):
            lanes = slice(0, PAIR if k == 0 else HD)
            total = None if first else partial[k, i, :, lanes]
            for zb in blocks:
                at = pl.ds(pl.multiple_of(zb * zpart, zpart), zpart)
                add = jnp.dot(tokens[i, :, at], wall[k, at, lanes], preferred_element_type=F32)
                total = add if total is None else total + add
            partial[k, i, :, lanes] = total

    def blocks_of(steps):
        return [ring_block(way, step + 1) for step in steps for way in range(2)]

    late = half_ring - 3
    for step in range(half_ring):
        for k in range(4):
            for way in range(2):
                if active(way, step, k):
                    ring(way, step, k, 1).wait_recv()
                    if active(way, step + 1, k):
                        ring(way, step + 1, k, 0).start()
                    if k >= 2:
                        pair_copy(way, step, k, odd).start()
            if step == late:
                project(k, [z] + blocks_of(range(late)), first=True)
            elif step > late:
                project(k, blocks_of((step - 1,)))
        if step == 2:
            token_gather.neighbours()
        if step == 4:
            token_gather.opposite()
        if step == late - 1:
            token_gather.arrived(token_ref(other))
    last_block = [ring_block(0, half_ring)]

    pieces = wo_send.shape[0]
    piece = width // pieces

    def w_out_ref(core, j):
        def ref(i, first, length):
            return wall.at[out_at + n_fs * core + i, pl.ds(j * piece + first, length), :]

        return ref

    w_out_gathers = [RowGather(w_out_ref(c, j), piece, wo_send, wo_recv, j) for j in range(pieces)]

    lanes_x = pl.ds(pl.multiple_of(x * HD, HD), HD)
    low = lax.broadcasted_iota(jnp.int32, (2 * own_rows, HD), 1) < HALF

    def unit(raw, gain):
        wide = raw.astype(BF16).astype(F32)
        square = wide * wide
        first = jnp.sum(jnp.where(low, square, 0.0), axis=-1, keepdims=True)
        second = jnp.sum(jnp.where(low, 0.0, square), axis=-1, keepdims=True)
        scale = jnp.where(low, lax.rsqrt(first / HALF + EPS), lax.rsqrt(second / HALF + EPS))
        return wide * scale * gain

    for i in range(n_fs):
        project(i, last_block)
        both = partial[0, i]
        query = (unit(both[:, :HD], q_gain_ref[:, lanes_x]) * HALF**-0.5).astype(BF16)
        key = unit(both[:, HD:], k_gain_ref[:, lanes_x]).astype(BF16)
        value = partial[1, i, :, 0:HD].astype(BF16)
        for s in range(own_seqs):
            for core in range(2):
                src = slice(core * own_rows + s * rows, core * own_rows + (s + 1) * rows)
                dst = slice(core * rows, (core + 1) * rows)
                qkv[own_seqs * i + s, dst, 0:HD] = query[src]
                qkv[own_seqs * i + s, dst, HD:PAIR] = key[src]
                qkv[own_seqs * i + s, dst, PAIR:] = value[src]

    def owner(zb):
        return lax.rem(lax.rem(zb, 2) + zb // 2, 2)

    def own_block(i):
        return 2 * i + lax.rem(i + c, 2)

    def other_block(i):
        return 2 * i + lax.rem(i + other, 2)

    offsets = [n_seq // 2]
    for d in range(n_seq // 2 - 1, 0, -1):
        offsets += [d, n_seq - d]
    my_owner = owner(z)

    def qkv_copy(n, offset):
        s = lax.rem(z // 2 + offset, n_seq)
        return copy(qkv.at[s], heads.at[z], a_send.at[n], a_recv.at[z // 2], sp=2 * s + c, tp=my_owner)

    for n, offset in enumerate(offsets):
        qkv_copy(n, offset).start()
    last = len(offsets)
    home = (c == lax.rem(z, 2)) & (my_owner == c)
    away = (c != lax.rem(z, 2)) | (my_owner != c)

    @pl.when(away)
    def _():
        qkv_copy(last, 0).start()

    @pl.when(home)
    def _():
        heads[z] = qkv[z // 2]

    for way, step, k in hops:
        pair_copy(way, step, k, 1 - odd).wait_recv()
    for gather in w_out_gathers:
        gather.own()

    @pl.loop(0, n_fs)
    def _(i):
        both = jnp.dot(tokens[i], wall[2], preferred_element_type=F32).astype(BF16)
        both = both.astype(F32)
        gate_b[i] = jnp.dot(tokens[i], wall[1, :, HD:PAIR], preferred_element_type=F32).astype(BF16)
        product = (both[:, :HD] * both[:, HD:]).astype(BF16).astype(F32)
        for s in range(own_seqs):
            for core in range(2):
                src = slice(core * own_rows + s * rows, core * own_rows + (s + 1) * rows)
                shaped[own_seqs * i + s, TAIL + core * rows : TAIL + (core + 1) * rows, :] = product[src]

    tail_copy = copy(
        shaped.at[:, block : block + TAIL, :],
        shaped.at[:, 0:TAIL, :],
        one_send.at[1],
        one_recv.at[1],
        sp=zr,
    )
    tail_copy.start()
    for gather in w_out_gathers:
        gather.neighbours()

    tail_copy.wait_recv()

    @pl.when(z == 0)
    def _():
        shaped[:, 0:TAIL, :] = jnp.zeros((n_seq, TAIL, HD), F32)

    taps = [taps_ref[i : i + 1, lanes_x] for i in range(3)]

    @pl.loop(0, n_fs)
    def _(i):
        for s in range(own_seqs):
            seq = own_seqs * i + s
            total = taps[0] * shaped[seq, TAIL - 2 : TAIL - 2 + block, :]
            total = total + taps[1] * shaped[seq, TAIL - 1 : TAIL - 1 + block, :]
            total = total + taps[2] * shaped[seq, TAIL : TAIL + block, :]
            for core in range(2):
                gate = gate_b[i, core * own_rows + s * rows : core * own_rows + (s + 1) * rows, :]
                gated = gate.astype(F32) * total[core * rows : (core + 1) * rows]
                conv[2 * i + core, s * rows : (s + 1) * rows, :] = gated.astype(BF16)

    def conv_copy(n, to, core):
        return copy(conv.at[2 * to + core], conv_all.at[me], c_send.at[n], c_recv.at[me], fs=to, tp=core)

    conv_to = [(xo, c), (xo, other), (xr, c), (xr, other), (xl, c), (xl, other), (x, other)]
    for n, (to, core) in enumerate(conv_to):
        conv_copy(n, to, core).start()
    conv_all[me] = conv[2 * x + c]


    def kv_copy(i, zb):
        ref = heads.at[zb, :, HD:]
        return copy(ref, ref, kv_send.at[i], kv_recv.at[i], tp=other)

    for i in range(n_seq):
        zb = own_block(i)

        @pl.when((zb != z) | (c != lax.rem(z, 2)))
        def _():
            copy(qkv.at[0], heads.at[zb], a_send.at[0], a_recv.at[i], sp=zb, tp=c).wait_recv()

        kv_copy(i, zb).start()
    for gather in w_out_gathers[:-1]:
        gather.opposite()
    lam_copy.wait_recv()
    for i in range(n_seq):
        kv_copy(i, other_block(i)).wait_recv()

    seq, mine = z // 2, lax.rem(z, 2)
    head = n_fs * mine + x
    seq_x, seq_row = seq // own_seqs, pl.ds(pl.multiple_of(lax.rem(seq, own_seqs) * rows, rows), rows)
    lane = lax.broadcasted_iota(jnp.int32, (block, HD), 1)
    key_at = lax.broadcasted_iota(jnp.int32, (2 * block, keys), 1)
    row_at = lax.rem(lax.broadcasted_iota(jnp.int32, (2 * block, keys), 0), block)

    def out_copy(i, zb, core):
        return copy(
            attn.at[i, core * rows : (core + 1) * rows, :],
            attn_all.at[head, seq_row, :],
            o_send.at[i, core],
            o_recv.at[head, lax.rem(seq, own_seqs)],
            fs=seq_x,
            sp=zb,
            tp=core,
        )

    def is_self(zb, core):
        return (seq_x == x) & (zb == z) & (c == core)

    def not_self(zb, core):
        return (seq_x != x) | (zb != z) | (c != core)

    def attend(i):
        zb = own_block(i)
        query = heads[zb, :, 0:HD].astype(F32)
        query = jnp.concatenate(
            [jnp.where(lane < HALF, query, 0.0), jnp.where(lane < HALF, 0.0, query)], axis=0
        ).astype(BF16)
        top = None
        for j in range(i + 1):
            key = heads[2 * j : 2 * j + 2, :, HD:PAIR].reshape(keys, HD)
            s = lax.dot_general(query, key, (((1,), (1,)), ((), ())), preferred_element_type=F32)
            if j == i:
                s = jnp.where(key_at <= row_at + block * lax.rem(i + c, 2), s, NEG)
            score[:, j * keys : (j + 1) * keys] = s
            best = functools.reduce(jnp.maximum, [s[:, n : n + HD] for n in range(0, keys, HD)] if keys >= HD else [s])
            top = best if top is None else jnp.maximum(top, best)
        top = jnp.max(top, axis=-1, keepdims=True)
        total, summed = None, None
        for j in range(i + 1):
            weight = jnp.exp(score[:, j * keys : (j + 1) * keys] - top)
            value = heads[2 * j : 2 * j + 2, :, PAIR:].reshape(keys, HD)
            add = jnp.dot(weight.astype(BF16), value, preferred_element_type=F32)
            w = sum(weight[:, n : n + HD] for n in range(0, keys, HD)) if keys >= HD else weight
            total = w if total is None else total + w
            summed = add if summed is None else summed + add
        maps = summed / jnp.sum(total, axis=-1, keepdims=True)
        differ = maps[:block] - lams[mine][0:1, :] * maps[block:]
        scale = lax.rsqrt(jnp.mean(differ * differ, axis=-1, keepdims=True) + EPS)
        attn[i] = (differ * scale * head_gain_ref[...] * OUT_SCALE).astype(BF16)
        for core in range(2):

            @pl.when(not_self(zb, core))
            def _():
                out_copy(i, zb, core).start()

            @pl.when(is_self(zb, core))
            def _():
                attn_all[head, seq_row, :] = attn[i, core * rows : (core + 1) * rows, :]

    @pl.loop(0, n_seq)
    def _(turn):
        now = lax.rem(z // 2 + turn, n_seq)
        for i in range(n_seq):

            @pl.when(now == i)
            def _():
                attend(i)

    w_out_gathers[-1].opposite()
    for j, gather in enumerate(w_out_gathers):
        gather.arrived(w_out_ref(other, j))
    for n, (to, core) in enumerate(conv_to):
        source = n_fs * core + to
        copy(conv.at[0], conv_all.at[source], c_send.at[n], c_recv.at[source], fs=to, tp=core).wait_recv()
    columns = min(width, 256)

    def projected(features, lanes, at):
        total = None
        for h in range(0, 2 * n_fs, 2):
            weight = jnp.concatenate([wall[out_at + h, at, lanes], wall[out_at + h + 1, at, lanes]], axis=1)
            add = lax.dot_general(
                jnp.concatenate([features[h], features[h + 1]], axis=1),
                weight,
                (((1,), (1,)), ((), ())),
                preferred_element_type=F32,
            )
            total = add if total is None else total + add
        return total

    @pl.loop(0, width // columns)
    def _(n):
        at = pl.ds(pl.multiple_of(n * columns, columns), columns)
        mixed[:, at] = projected(conv_all, slice(HD, PAIR), at)

    for h in range(2 * n_fs):
        for s in range(own_seqs):
            source_x, source_z = h % n_fs, 2 * (own_seqs * x + s) + h // n_fs

            @pl.when((source_x != x) | (source_z != z) | (my_owner != c))
            def _():
                copy(
                    attn.at[0, 0:rows, :],
                    attn_all.at[h, s * rows : (s + 1) * rows, :],
                    o_send.at[0, 0],
                    o_recv.at[h, s],
                    fs=source_x,
                    sp=source_z,
                    tp=my_owner,
                ).wait_recv()

    @pl.loop(0, width // columns)
    def _(n):
        at = pl.ds(pl.multiple_of(n * columns, columns), columns)
        total = mixed[:, at] + projected(attn_all, slice(0, HD), at)
        for s in range(own_seqs):
            out_ref[s, :, at] = total[s * rows : (s + 1) * rows].astype(BF16)

    for k in range(4):
        for n, to in enumerate((xr, xl, xo)):
            shard_copy(k, n, to, x).wait_send()
    for way, step, k in hops:
        pair_copy(way, step, k, odd).wait_send()
    for step in range(half_ring):
        for k in range(4):
            for way in range(2):
                if active(way, step, k):
                    ring(way, step, k, 0).wait_send()
    token_gather.sent()
    for gather in w_out_gathers:
        gather.sent()
    lam_copy.wait_send()
    tail_copy.wait_send()
    for n, offset in enumerate(offsets):
        qkv_copy(n, offset).wait_send()

    @pl.when(away)
    def _():
        qkv_copy(last, 0).wait_send()

    for n, (to, core) in enumerate(conv_to):
        conv_copy(n, to, core).wait_send()
    for i in range(n_seq):
        zb = own_block(i)
        kv_copy(i, zb).wait_send()
        for core in range(2):

            @pl.when(not_self(zb, core))
            def _():
                out_copy(i, zb, core).wait_send()


def on_device(n_grp, n_sp, n_fs, *args):
    tokens, norm_gain, wq, wk, wv, q_gain, k_gain, lam, head_gain, wb, wc, wi, taps, woa, woc = args
    own_seqs, rows, width = tokens.shape
    n_seq, block, n_head = own_seqs * n_fs, 2 * rows, 2 * n_fs
    assert n_grp % 2 == 0 and n_sp == 2 * n_seq and n_fs == 4 and own_seqs == 2
    half_ring = n_sp // 2
    row = lambda v: v.reshape(1, -1)
    ins = (
        tokens, row(norm_gain), wq, wk, wv, row(q_gain), row(k_gain), row(lam), row(head_gain),
        wb, wc, wi, taps, woa.T, woc.T,
    )
    dma = pltpu.SemaphoreType.DMA
    vmem = pl.BlockSpec(memory_space=pltpu.VMEM)
    call = pl.pallas_call(
        functools.partial(kernel, n_grp, n_sp, n_fs),
        out_shape=jax.ShapeDtypeStruct(tokens.shape, BF16),
        in_specs=[pl.BlockSpec(memory_space=pltpu.HBM)] * 15,
        out_specs=vmem,
        scratch_shapes=[pltpu.VMEM(a.shape, a.dtype) for a in ins]
        + [
            pltpu.VMEM((n_fs, 2 * own_seqs * rows, width), BF16),
            pltpu.VMEM((n_fs, 4, wq.shape[0], PAIR), BF16),
            pltpu.VMEM((3 + n_head, width, PAIR), BF16),
            pltpu.VMEM((2, n_fs, 2 * own_seqs * rows, PAIR), F32),
            pltpu.VMEM((n_seq, block, 3 * HD), BF16),
            pltpu.VMEM((n_fs, 2 * own_seqs * rows, HD), BF16),
            pltpu.VMEM((n_sp, block, 3 * HD), BF16),
            pltpu.VMEM((2 * block, n_sp * block), F32),
            pltpu.VMEM((n_seq, block, HD), BF16),
            pltpu.VMEM((n_head, own_seqs * rows, HD), BF16),
            pltpu.VMEM((n_seq, TAIL + block, HD), F32),
            pltpu.VMEM((n_head, own_seqs * rows, HD), BF16),
            pltpu.VMEM((n_head, own_seqs * rows, HD), BF16),
            pltpu.VMEM((2, 8, HD), F32),
            pltpu.VMEM((own_seqs * rows, width), F32),
            dma((3, 4)),
            dma((3, 4)),
            dma((1, 8)),
            dma((1, 8)),
            dma((2, half_ring, 4)),
            dma((2, half_ring, 4)),
            dma((2, 2, half_ring)),
            dma((2, 2, half_ring)),
            pltpu.SemaphoreType.REGULAR,
            dma((n_seq,)),
            dma((n_seq,)),
            dma((n_seq,)),
            dma((n_seq,)),
            dma((n_seq, 2)),
            dma((n_head, own_seqs)),
            dma((n_head,)),
            dma((n_head,)),
            dma((4, 8)),
            dma((4, 8)),
            dma((2,)),
            dma((2,)),
            dma((15,)),
        ],
        compiler_params=pltpu.CompilerParams(
            collective_id=0, has_side_effects=True, vmem_limit_bytes=32 * 1024 * 1024
        ),
    )
    return call(*[pltpu.with_memory_space_constraint(a, pltpu.HBM) for a in ins])


def solution(mesh):
    placed = (
        P(("grp", "fs"), ("sp", "tp"), None),
        P(),
        P(("sp", "fs"), "tp"),
        P(("sp", "fs"), "tp"),
        P(("sp", "fs"), "tp"),
        P("tp"),
        P("tp"),
        P("tp"),
        P(),
        P(("sp", "fs"), "tp"),
        P(("sp", "fs"), "tp"),
        P(("sp", "fs"), "tp"),
        P(None, "tp"),
        P("tp", ("sp", "fs")),
        P("tp", ("sp", "fs")),
    )
    return jax.shard_map(
        functools.partial(on_device, mesh.shape["grp"], mesh.shape["sp"], mesh.shape["fs"]),
        mesh=mesh,
        in_specs=placed,
        out_specs=P(("grp", "fs"), ("sp", "tp"), None),
        check_vma=False,
    )
```

```python
import functools

import jax
import jax.numpy as jnp
from jax import lax
from jax.experimental import pallas as pl
from jax.experimental.pallas import tpu as pltpu
from jax.sharding import PartitionSpec as P

EPS = 1e-06
NEG = -1e30
OUT_SCALE = 0.8
HD = 128
HALF = HD // 2
PAIR = 2 * HD
TAIL = 8
F32 = jnp.float32
BF16 = jnp.bfloat16
MESH = pl.DeviceIdType.MESH


def kernel(
    n_grp,
    n_sp,
    n_fs,
    *refs,
):
    (tok_ref, norm_gain_ref, wq_ref, wk_ref, wv_ref, q_gain_ref, k_gain_ref, lam_ref, head_gain_ref, wb_ref, wc_ref, wi_ref, taps_ref, woa_ref, woc_ref) = refs[16:31]
    (
    out_ref,
    tokens,
    stage,
    wall,
    partial,
    qkv,
    gate_b,
    heads,
    score,
    attn,
    attn_all,
    shaped,
    conv,
    conv_all,
    lams,
    mixed,
    send,
    w_recv,
    t_recv,
    ring_recv,
    pair_recv,
    ready,
    a_recv,
    kv_recv,
    o_recv,
    c_recv,
    wo_recv,
    one_send,
    one_recv,
    load_sem,
    ) = (refs[15], *refs[31:])
    weights, others = (2, 3, 4, 9, 10, 11, 13, 14), (0, 1, 5, 6, 7, 8, 12)
    load_at = {n: 0 for n in weights} | {n: 1 + i for i, n in enumerate(others)}
    loads = [pltpu.make_async_copy(refs[n], refs[16 + n], load_sem.at[load_at[n]]) for n in range(15)]
    for n in weights + others:
        loads[n].start()
    g = lax.axis_index("grp")
    z, x, c = lax.axis_index("sp"), lax.axis_index("fs"), lax.axis_index("tp")
    own_seqs, rows, width = tok_ref.shape
    own_rows = own_seqs * rows
    block = 2 * rows
    keys = 2 * block
    part = wq_ref.shape[0]
    zpart = n_fs * part
    n_seq = own_seqs * n_fs
    half_ring = n_sp // 2
    xr, xl, xo = lax.rem(x + 1, n_fs), lax.rem(x + n_fs - 1, n_fs), lax.rem(x + 2, n_fs)
    zr, zl = lax.rem(z + 1, n_sp), lax.rem(z + n_sp - 1, n_sp)
    other = 1 - c
    me = n_fs * c + x
    odd = lax.rem(g, 2)
    pair = g + 1 - 2 * odd
    out_at = 3

    def copy(src, dst, send, recv, **where):
        return pltpu.make_async_remote_copy(
            src_ref=src,
            dst_ref=dst,
            send_sem=send,
            recv_sem=recv,
            device_id=where,
            device_id_type=MESH,
        )

    def together(sem, size):
        lines = size // (2 * PAIR)
        for most in range(1, wall.shape[0] + 1):
            if lines % most == 0 and lines // most <= width and lines // most % 16 == 0:
                ref = wall.at[0:most, 0 : lines // most, :]
                return copy(ref, ref, sem, sem, tp=other)
        raise ValueError(size)

    shard_size, slice_size = part * 2 * PAIR, zpart * 2 * PAIR
    token_size, conv_size = own_rows * width * 2, own_rows * HD * 2
    out_size, kv_size = rows * HD * 2, block * 2 * PAIR

    barrier = pltpu.get_barrier_semaphore()
    near = [dict(fs=xr), dict(fs=xl), dict(fs=xo), dict(tp=other), dict(sp=zl), dict(grp=pair)]
    for where in near:
        pl.semaphore_signal(barrier, inc=1, device_id=where, device_id_type=MESH)

    pltpu.make_async_copy(stage, stage, load_sem.at[0]).wait()
    for n in others:
        loads[n].wait()

    sides = ((wq_ref, wk_ref), (wv_ref, wb_ref), (wc_ref, wi_ref), (woa_ref, woc_ref))
    for to in range(n_fs):
        lanes = slice(to * HD, (to + 1) * HD)
        for k, (left, right) in enumerate(sides):
            stage[to, k, :, 0:HD] = left[:, lanes]
            stage[to, k, :, HD:PAIR] = right[:, lanes]
    pl.semaphore_wait(barrier, len(near))

    pl.semaphore_signal(ready, inc=1, device_id=dict(sp=zr), device_id_type=MESH)

    def chunk_at(k, to):
        return out_at + n_fs * c + to if k == 3 else k

    def shard_copy(k, n, to, source):
        at = pl.ds(pl.multiple_of(z * zpart + source * part, part), part)
        return copy(stage.at[to, k], wall.at[chunk_at(k, to), at, :], send.at[0], w_recv.at[k], fs=to)

    for k in range(4):
        for n, to in ((2, xo), (0, xr), (1, xl)):
            shard_copy(k, n, to, x).start()
    here = pl.ds(pl.multiple_of(z * zpart + x * part, part), part)
    wall[0:3, here, :] = stage[x, 0:3]
    wall[out_at + me, here, :] = stage[x, 3]

    step_rows = min(rows, 32)
    for s in range(own_seqs):
        for r in range(0, rows, step_rows):
            wide = tok_ref[s, r : r + step_rows, :].astype(F32)
            scale = lax.rsqrt(jnp.mean(wide * wide, axis=-1, keepdims=True) + EPS)
            at = pl.multiple_of(c * own_rows + s * rows + r, step_rows)
            tokens[x, pl.ds(at, step_rows), :] = (wide * scale * norm_gain_ref[...]).astype(BF16)

    class RowGather:
        def __init__(self, ref, size, send, recv, j):
            self.ref, self.size, self.send, self.recv, self.j = ref, size, send, recv, j

        def one(self, n, i, part_of, **where):
            first, length = ((0, self.size), (0, self.size // 2), (self.size // 2, self.size // 2))[part_of]
            ref = self.ref(i, first, length)
            return copy(ref, ref, self.send, self.recv.at[self.j if n < 4 else 0, min(n, 4)], **where)

        def sent_as(self, n):
            i, part_of, where = (
                (x, 0, dict(fs=xr)),
                (x, 0, dict(fs=xl)),
                (xl, 1, dict(fs=xr)),
                (xr, 2, dict(fs=xl)),
                (x, 0, dict(tp=other)),
                (xl, 0, dict(tp=other)),
                (xr, 0, dict(tp=other)),
                (xo, 0, dict(tp=other)),
            )[n]
            return self.one(n, i, part_of, **where)

        def own(self):
            for n in (0, 1, 4):
                self.sent_as(n).start()

        def neighbours(self):
            self.one(0, xl, 0, fs=xr).wait_recv()
            self.sent_as(2).start()
            self.one(1, xr, 0, fs=xl).wait_recv()
            for n in (3, 5, 6):
                self.sent_as(n).start()

        def opposite(self):
            self.one(2, xo, 1, fs=xr).wait_recv()
            self.one(3, xo, 2, fs=xl).wait_recv()
            self.sent_as(7).start()

    def token_ref(core):
        def ref(i, first, length):
            return tokens.at[i, pl.ds(pl.multiple_of(core * own_rows + first, length), length), :]

        return ref

    token_gather = RowGather(token_ref(c), own_rows, send.at[1], t_recv, 0)

    lane = lax.broadcasted_iota(jnp.int32, lam_ref.shape, 1)
    chosen = jnp.sum(jnp.where(lane == x, lam_ref[...], 0.0), axis=-1, keepdims=True)
    lams[c] = jnp.broadcast_to(chosen, lams.shape[1:])
    lam_copy = copy(lams.at[c], lams.at[c], one_send.at[0], one_recv.at[0], tp=other)
    lam_copy.start()

    pieces_of = ((0, 0, 2), (0, 1, 2), (1, 0, 1), (2, 0, 2), (2, 1, 2), (3, 0, 2))

    def slice_ref(k, zb, side):
        kind, nth, count = pieces_of[k]
        length = zpart // count
        first = zb * zpart + (side if kind == 3 else nth) * length
        at = pl.ds(pl.multiple_of(first, length), length)
        if kind == 2:
            return wall.at[2 + side * (1 + me), at, :]
        return wall.at[(0, 1, 2, 1)[kind], at, (slice(0, PAIR), slice(0, HD), None, slice(HD, PAIR))[kind]]

    def ring_block(way, step):
        return lax.rem(z - step + 2 * n_sp, n_sp) if way == 0 else lax.rem(z + step, n_sp)

    def ring(way, step, k, ahead):
        ref = slice_ref(k, ring_block(way, step + ahead), odd)
        to = zr if way == 0 else zl
        return copy(ref, ref, send.at[2], ring_recv.at[way, step, k], sp=to)

    def pair_copy(way, step, k, side):
        ref = slice_ref(k, ring_block(way, step + 1), side)
        return copy(ref, ref, send.at[3], pair_recv.at[k // 5], grp=pair)

    def active(way, step, k):
        return step < half_ring - 1 or (step == half_ring - 1 and (k in (0, 1, 5)) == (way == 0))

    @pl.when(z != 0)
    def _():
        pl.semaphore_wait(ready, 1)

    for k in range(4):
        together(w_recv.at[k], 3 * shard_size).wait_recv()
        for slot, its in enumerate((0, 0, 1, 3, 3, 1)):
            if k == its:
                ring(0, 0, slot, 0).start()

                @pl.when(z != 0)
                def _():
                    ring(1, 0, slot, 0).start()

    token_gather.own()
    @pl.when(z == 0)
    def _():
        pl.semaphore_wait(ready, 1)
        for k in range(6):
            ring(1, 0, k, 0).start()

    def project(i, blocks, first=False):
        for k in range(2):
            lanes = slice(0, PAIR if k == 0 else HD)
            total = None if first else partial[k, i, :, lanes]
            for zb in blocks:
                at = pl.ds(pl.multiple_of(zb * zpart, zpart), zpart)
                add = jnp.dot(tokens[i, :, at], wall[k, at, lanes], preferred_element_type=F32)
                total = add if total is None else total + add
            partial[k, i, :, lanes] = total

    def blocks_of(steps):
        return [ring_block(way, step + 1) for step in steps for way in range(2)]

    late = half_ring - 3
    for step in range(half_ring):
        for k in range(6):
            for way in range(2):
                if active(way, step, k):
                    ring(way, step, k, 1).wait_recv()
                    if active(way, step + 1, k):
                        ring(way, step + 1, k, 0).start()
                    if k >= 3:
                        pair_copy(way, step, k, odd).start()
            if k >= n_fs:
                continue
            if step == late:
                project(k, [z] + blocks_of(range(late)), first=True)
            elif step > late:
                project(k, blocks_of((step - 1,)))
        if step == 3:
            token_gather.neighbours()
        if step == 4:
            token_gather.opposite()
        if step == late - 1:
            together(t_recv.at[0, 4], n_fs * token_size).wait_recv()
    last_block = [ring_block(0, half_ring)]

    pieces = wo_recv.shape[0]
    piece = width // pieces

    def w_out_ref(core, j):
        def ref(i, first, length):
            return wall.at[out_at + n_fs * core + i, pl.ds(j * piece + first, length), :]

        return ref

    w_out_gathers = [RowGather(w_out_ref(c, j), piece, send.at[5], wo_recv, j) for j in range(pieces)]

    lanes_x = pl.ds(pl.multiple_of(x * HD, HD), HD)
    low = lax.broadcasted_iota(jnp.int32, (2 * own_rows, HD), 1) < HALF

    def unit(raw, gain):
        wide = raw.astype(BF16).astype(F32)
        square = wide * wide
        first = jnp.sum(jnp.where(low, square, 0.0), axis=-1, keepdims=True)
        second = jnp.sum(jnp.where(low, 0.0, square), axis=-1, keepdims=True)
        scale = jnp.where(low, lax.rsqrt(first / HALF + EPS), lax.rsqrt(second / HALF + EPS))
        return wide * scale * gain

    for i in range(n_fs):
        project(i, last_block)
        both = partial[0, i]
        query = (unit(both[:, :HD], q_gain_ref[:, lanes_x]) * HALF**-0.5).astype(BF16)
        key = unit(both[:, HD:], k_gain_ref[:, lanes_x]).astype(BF16)
        value = partial[1, i, :, 0:HD].astype(BF16)
        for s in range(own_seqs):
            for core in range(2):
                src = slice(core * own_rows + s * rows, core * own_rows + (s + 1) * rows)
                dst = slice(core * rows, (core + 1) * rows)
                qkv[own_seqs * i + s, dst, 0:HD] = query[src]
                qkv[own_seqs * i + s, dst, HD:PAIR] = key[src]
                qkv[own_seqs * i + s, dst, PAIR:] = value[src]

    def owner(zb):
        return lax.rem(lax.rem(zb, 2) + zb // 2, 2)

    def own_block(i):
        return 2 * i + lax.rem(i + c, 2)

    def other_block(i):
        return 2 * i + lax.rem(i + other, 2)

    offsets = [n_seq // 2]
    for d in range(n_seq // 2 - 1, 0, -1):
        offsets += [d, n_seq - d]
    my_owner = owner(z)

    last = len(offsets)

    def qkv_copy(n, offset):
        s = lax.rem(z // 2 + offset, n_seq)
        return copy(qkv.at[s], heads.at[z], send.at[4 if n < last else 9], a_recv.at[z // 2], sp=2 * s + c, tp=my_owner)

    for n, offset in enumerate(offsets):
        qkv_copy(n, offset).start()
    home = (c == lax.rem(z, 2)) & (my_owner == c)
    away = (c != lax.rem(z, 2)) | (my_owner != c)

    @pl.when(away)
    def _():
        qkv_copy(last, 0).start()

    @pl.when(home)
    def _():
        heads[z] = qkv[z // 2]

    together(pair_recv.at[0], (n_sp - 1) * slice_size).wait_recv()
    together(pair_recv.at[1], (n_sp - 1) * slice_size // 4).wait_recv()
    for gather in w_out_gathers:
        gather.own()

    @pl.loop(0, n_fs)
    def _(i):
        both = jnp.dot(tokens[i], wall[2], preferred_element_type=F32).astype(BF16)
        both = both.astype(F32)
        gate_b[i] = jnp.dot(tokens[i], wall[1, :, HD:PAIR], preferred_element_type=F32).astype(BF16)
        product = (both[:, :HD] * both[:, HD:]).astype(BF16).astype(F32)
        for s in range(own_seqs):
            for core in range(2):
                src = slice(core * own_rows + s * rows, core * own_rows + (s + 1) * rows)
                shaped[own_seqs * i + s, TAIL + core * rows : TAIL + (core + 1) * rows, :] = product[src]

    tail_copy = copy(
        shaped.at[:, block : block + TAIL, :],
        shaped.at[:, 0:TAIL, :],
        one_send.at[1],
        one_recv.at[1],
        sp=zr,
    )
    tail_copy.start()
    for gather in w_out_gathers:
        gather.neighbours()

    def kv_copy(i, zb):
        ref = heads.at[zb, :, HD:]
        return copy(ref, ref, send.at[7], kv_recv.at[0], tp=other)

    for i in range(n_seq):
        zb = own_block(i)

        @pl.when((zb != z) | (c != lax.rem(z, 2)))
        def _():
            copy(qkv.at[0], heads.at[zb], send.at[4], a_recv.at[i], sp=zb, tp=c).wait_recv()

        kv_copy(i, zb).start()
    tail_copy.wait_recv()

    @pl.when(z == 0)
    def _():
        shaped[:, 0:TAIL, :] = jnp.zeros((n_seq, TAIL, HD), F32)

    taps = [taps_ref[i : i + 1, lanes_x] for i in range(3)]

    @pl.loop(0, n_fs)
    def _(i):
        for s in range(own_seqs):
            seq = own_seqs * i + s
            total = taps[0] * shaped[seq, TAIL - 2 : TAIL - 2 + block, :]
            total = total + taps[1] * shaped[seq, TAIL - 1 : TAIL - 1 + block, :]
            total = total + taps[2] * shaped[seq, TAIL : TAIL + block, :]
            for core in range(2):
                gate = gate_b[i, core * own_rows + s * rows : core * own_rows + (s + 1) * rows, :]
                gated = gate.astype(F32) * total[core * rows : (core + 1) * rows]
                conv[2 * i + core, s * rows : (s + 1) * rows, :] = gated.astype(BF16)

    def conv_copy(n, to, core):
        return copy(conv.at[2 * to + core], conv_all.at[me], send.at[6], c_recv.at[0], fs=to, tp=core)

    conv_to = [(xo, c), (xo, other), (xr, c), (xr, other), (xl, c), (xl, other), (x, other)]
    for n, (to, core) in enumerate(conv_to):
        conv_copy(n, to, core).start()
    conv_all[me] = conv[2 * x + c]


    for gather in w_out_gathers[:-1]:
        gather.opposite()
    lam_copy.wait_recv()
    together(kv_recv.at[0], n_seq * kv_size).wait_recv()

    seq, mine = z // 2, lax.rem(z, 2)
    head = n_fs * mine + x
    seq_x, seq_row = seq // own_seqs, pl.ds(pl.multiple_of(lax.rem(seq, own_seqs) * rows, rows), rows)
    lane = lax.broadcasted_iota(jnp.int32, (block, HD), 1)
    key_at = lax.broadcasted_iota(jnp.int32, (2 * block, keys), 1)
    row_at = lax.rem(lax.broadcasted_iota(jnp.int32, (2 * block, keys), 0), block)

    def out_copy(i, zb, core):
        return copy(
            attn.at[i, core * rows : (core + 1) * rows, :],
            attn_all.at[head, seq_row, :],
            send.at[8],
            o_recv.at[head // 2],
            fs=seq_x,
            sp=zb,
            tp=core,
        )

    def is_self(zb, core):
        return (seq_x == x) & (zb == z) & (c == core)

    def not_self(zb, core):
        return (seq_x != x) | (zb != z) | (c != core)

    def scored(i, first):
        zb = own_block(i)
        query = heads[zb, :, 0:HD].astype(F32)
        query = jnp.concatenate(
            [jnp.where(lane < HALF, query, 0.0), jnp.where(lane < HALF, 0.0, query)], axis=0
        ).astype(BF16)
        top = None
        for j in range(i + 1):
            key = heads[2 * j : 2 * j + 2, :, HD:PAIR].reshape(keys, HD)
            s = lax.dot_general(query, key, (((1,), (1,)), ((), ())), preferred_element_type=F32)
            if j == i:
                s = jnp.where(key_at <= row_at + block * lax.rem(i + c, 2), s, NEG)
            score[:, first + j * keys : first + (j + 1) * keys] = s
            top = folded(jnp.maximum, s, top)
        return jnp.max(top, axis=-1, keepdims=True)

    def folded(op, s, start):
        for n in range(0, keys, min(HD, keys)):
            piece = s[:, n : n + min(HD, keys)]
            start = piece if start is None else op(start, piece)
        return start

    def weighted(i, first, top):
        total, summed = None, None
        for j in range(i + 1):
            weight = jnp.exp(score[:, first + j * keys : first + (j + 1) * keys] - top)
            value = heads[2 * j : 2 * j + 2, :, PAIR:].reshape(keys, HD)
            add = jnp.dot(weight.astype(BF16), value, preferred_element_type=F32)
            total = folded(jnp.add, weight, total)
            summed = add if summed is None else summed + add
        return summed, jnp.sum(total, axis=-1, keepdims=True)

    def finished(i, summed, total):
        maps = summed / total
        differ = maps[:block] - lams[mine][0:1, :] * maps[block:]
        scale = lax.rsqrt(jnp.mean(differ * differ, axis=-1, keepdims=True) + EPS)
        attn[i] = (differ * scale * head_gain_ref[...] * OUT_SCALE).astype(BF16)

    def deliver(i):
        zb = own_block(i)
        for core in range(2):

            @pl.when(not_self(zb, core))
            def _():
                out_copy(i, zb, core).start()

            @pl.when(is_self(zb, core))
            def _():
                attn_all[head, seq_row, :] = attn[i, core * rows : (core + 1) * rows, :]

    @pl.loop(0, n_seq // 2)
    def _(turn):
        now = lax.rem(z // 2 + turn, n_seq // 2)
        for p in range(n_seq // 2):

            @pl.when(now == p)
            def _():
                both = ((n_seq - 1 - p, 0), (p, n_sp * block))
                tops = [scored(i, first) for i, first in both]
                sums = [weighted(i, first, top) for (i, first), top in zip(both, tops)]
                for (i, _), (summed, total) in zip(both, sums):
                    finished(i, summed, total)
                for i, _ in both:
                    deliver(i)

    w_out_gathers[-1].opposite()
    together(wo_recv.at[0, 4], n_fs * width * 2 * PAIR).wait_recv()
    together(c_recv.at[0], len(conv_to) * conv_size).wait_recv()
    columns = min(width, 256)

    def projected(features, lanes, at, h):
        weight = jnp.concatenate([wall[out_at + h, at, lanes], wall[out_at + h + 1, at, lanes]], axis=1)
        pair_of = jnp.concatenate([features[h], features[h + 1]], axis=1)
        return lax.dot_general(pair_of, weight, (((1,), (1,)), ((), ())), preferred_element_type=F32)

    def column(n):
        return pl.ds(pl.multiple_of(n * columns, columns), columns)

    @pl.loop(0, width // columns)
    def _(n):
        at = column(n)
        mixed[:, at] = sum(projected(conv_all, slice(HD, PAIR), at, h) for h in range(0, 2 * n_fs, 2))

    kept = (seq_x == x) & (my_owner == c)
    sent_all = (seq_x != x) | (my_owner != c)
    for h in range(0, 2 * n_fs, 2):
        here_too = kept & (head // 2 == h // 2)
        not_here = sent_all | (head // 2 != h // 2)

        @pl.when(here_too)
        def _():
            together(o_recv.at[h // 2], (2 * own_seqs - 1) * out_size).wait_recv()

        @pl.when(not_here)
        def _():
            together(o_recv.at[h // 2], 2 * own_seqs * out_size).wait_recv()

        if h < 2 * n_fs - 2:

            @pl.loop(0, width // columns)
            def _(n):
                at = column(n)
                mixed[:, at] += projected(attn_all, slice(0, HD), at, h)

    @pl.loop(0, width // columns)
    def _(n):
        at = column(n)
        total = mixed[:, at] + projected(attn_all, slice(0, HD), at, 2 * n_fs - 2)
        for s in range(own_seqs):
            out_ref[s, :, at] = total[s * rows : (s + 1) * rows].astype(BF16)

    together(send.at[0], 12 * shard_size).wait_send()
    together(send.at[1], 7 * token_size).wait_send()
    together(send.at[2], (n_sp - 1) * slice_size * 11 // 4).wait_send()
    together(send.at[3], (n_sp - 1) * slice_size * 5 // 4).wait_send()
    together(send.at[4], last * block * 6 * HD).wait_send()
    together(send.at[5], 7 * width * 2 * PAIR).wait_send()
    together(send.at[6], len(conv_to) * conv_size).wait_send()
    together(send.at[7], n_seq * kv_size).wait_send()
    lam_copy.wait_send()
    tail_copy.wait_send()

    @pl.when(away)
    def _():
        qkv_copy(last, 0).wait_send()

    @pl.when(kept)
    def _():
        together(send.at[8], (2 * n_seq - 1) * out_size).wait_send()

    @pl.when(sent_all)
    def _():
        together(send.at[8], 2 * n_seq * out_size).wait_send()


def on_device(n_grp, n_sp, n_fs, *args):
    tokens, norm_gain, wq, wk, wv, q_gain, k_gain, lam, head_gain, wb, wc, wi, taps, woa, woc = args
    own_seqs, rows, width = tokens.shape
    n_seq, block, n_head = own_seqs * n_fs, 2 * rows, 2 * n_fs
    assert n_grp % 2 == 0 and n_sp == 2 * n_seq and n_fs == 4 and own_seqs == 2
    half_ring = n_sp // 2
    row = lambda v: v.reshape(1, -1)
    ins = (
        tokens, row(norm_gain), wq, wk, wv, row(q_gain), row(k_gain), row(lam), row(head_gain),
        wb, wc, wi, taps, woa.T, woc.T,
    )
    dma = pltpu.SemaphoreType.DMA
    vmem = pl.BlockSpec(memory_space=pltpu.VMEM)
    call = pl.pallas_call(
        functools.partial(kernel, n_grp, n_sp, n_fs),
        out_shape=jax.ShapeDtypeStruct(tokens.shape, BF16),
        in_specs=[pl.BlockSpec(memory_space=pltpu.HBM)] * 15,
        out_specs=vmem,
        scratch_shapes=[pltpu.VMEM(a.shape, a.dtype) for a in ins]
        + [
            pltpu.VMEM((n_fs, 2 * own_seqs * rows, width), BF16),
            pltpu.VMEM((n_fs, 4, wq.shape[0], PAIR), BF16),
            pltpu.VMEM((3 + n_head, width, PAIR), BF16),
            pltpu.VMEM((2, n_fs, 2 * own_seqs * rows, PAIR), F32),
            pltpu.VMEM((n_seq, block, 3 * HD), BF16),
            pltpu.VMEM((n_fs, 2 * own_seqs * rows, HD), BF16),
            pltpu.VMEM((n_sp, block, 3 * HD), BF16),
            pltpu.VMEM((2 * block, n_sp * block * 3 // 2), F32),
            pltpu.VMEM((n_seq, block, HD), BF16),
            pltpu.VMEM((n_head, own_seqs * rows, HD), BF16),
            pltpu.VMEM((n_seq, TAIL + block, HD), F32),
            pltpu.VMEM((n_head, own_seqs * rows, HD), BF16),
            pltpu.VMEM((n_head, own_seqs * rows, HD), BF16),
            pltpu.VMEM((2, 8, HD), F32),
            pltpu.VMEM((own_seqs * rows, width), F32),
            dma((10,)),
            dma((4,)),
            dma((1, 5)),
            dma((2, half_ring, 6)),
            dma((2,)),
            pltpu.SemaphoreType.REGULAR,
            dma((n_seq,)),
            dma((1,)),
            dma((n_fs,)),
            dma((1,)),
            dma((4, 5)),
            dma((2,)),
            dma((2,)),
            dma((8,)),
        ],
        compiler_params=pltpu.CompilerParams(
            collective_id=0, has_side_effects=True, vmem_limit_bytes=32 * 1024 * 1024
        ),
    )
    return call(*[pltpu.with_memory_space_constraint(a, pltpu.HBM) for a in ins])


def solution(mesh):
    placed = (
        P(("grp", "fs"), ("sp", "tp"), None),
        P(),
        P(("sp", "fs"), "tp"),
        P(("sp", "fs"), "tp"),
        P(("sp", "fs"), "tp"),
        P("tp"),
        P("tp"),
        P("tp"),
        P(),
        P(("sp", "fs"), "tp"),
        P(("sp", "fs"), "tp"),
        P(("sp", "fs"), "tp"),
        P(None, "tp"),
        P("tp", ("sp", "fs")),
        P("tp", ("sp", "fs")),
    )
    return jax.shard_map(
        functools.partial(on_device, mesh.shape["grp"], mesh.shape["sp"], mesh.shape["fs"]),
        mesh=mesh,
        in_specs=placed,
        out_specs=P(("grp", "fs"), ("sp", "tp"), None),
        check_vma=False,
    )
```

```python
import functools

import jax
import jax.numpy as jnp
from jax import lax
from jax.experimental import pallas as pl
from jax.experimental.pallas import tpu as pltpu
from jax.sharding import PartitionSpec as P

EPS = 1e-06
NEG = -1e30
OUT_SCALE = 0.8
HD = 128
HALF = HD // 2
PAIR = 2 * HD
LATE = 2
TAIL = 8
F32 = jnp.float32
BF16 = jnp.bfloat16
MESH = pl.DeviceIdType.MESH


def kernel(
    n_grp,
    n_sp,
    n_fs,
    *refs,
):
    (tok_ref, norm_gain_ref, wq_ref, wk_ref, wv_ref, q_gain_ref, k_gain_ref, lam_ref, head_gain_ref, wb_ref, wc_ref, wi_ref, taps_ref, woa_ref, woc_ref) = refs[16:31]
    (
    out_ref,
    tokens,
    stage,
    wall,
    partial,
    qkv,
    gate_b,
    heads,
    score,
    attn,
    attn_all,
    shaped,
    conv,
    conv_all,
    lams,
    mixed,
    send,
    w_recv,
    t_recv,
    ring_recv,
    pair_recv,
    ready,
    a_recv,
    kv_recv,
    o_recv,
    c_recv,
    wo_recv,
    one_send,
    one_recv,
    load_sem,
    ) = (refs[15], *refs[31:])
    weights, others = (2, 3, 4, 9, 10, 11, 13, 14), (0, 1, 5, 6, 7, 8, 12)
    load_at = {n: 0 for n in weights} | {n: 1 + i for i, n in enumerate(others)}
    loads = [pltpu.make_async_copy(refs[n], refs[16 + n], load_sem.at[load_at[n]]) for n in range(15)]
    for n in weights + others:
        loads[n].start()
    g = lax.axis_index("grp")
    z, x, c = lax.axis_index("sp"), lax.axis_index("fs"), lax.axis_index("tp")
    own_seqs, rows, width = tok_ref.shape
    own_rows = own_seqs * rows
    block = 2 * rows
    keys = 2 * block
    part = wq_ref.shape[0]
    zpart = n_fs * part
    n_seq = own_seqs * n_fs
    half_ring = n_sp // 2
    xr, xl, xo = lax.rem(x + 1, n_fs), lax.rem(x + n_fs - 1, n_fs), lax.rem(x + 2, n_fs)
    zr, zl = lax.rem(z + 1, n_sp), lax.rem(z + n_sp - 1, n_sp)
    other = 1 - c
    me = n_fs * c + x
    odd = lax.rem(g, 2)
    pair = g + 1 - 2 * odd
    out_at = 3

    def copy(src, dst, send, recv, **where):
        return pltpu.make_async_remote_copy(
            src_ref=src,
            dst_ref=dst,
            send_sem=send,
            recv_sem=recv,
            device_id=where,
            device_id_type=MESH,
        )

    def together(sem, size):
        lines = size // (2 * PAIR)
        for most in range(1, wall.shape[0] + 1):
            if lines % most == 0 and lines // most <= width and lines // most % 16 == 0:
                ref = wall.at[0:most, 0 : lines // most, :]
                return copy(ref, ref, sem, sem, tp=other)
        raise ValueError(size)

    shard_size, slice_size = part * 2 * PAIR, zpart * 2 * PAIR
    token_size, conv_size = own_rows * width * 2, own_rows * HD * 2
    out_size, kv_size = rows * HD * 2, block * 2 * PAIR

    barrier = pltpu.get_barrier_semaphore()
    near = [dict(fs=xr), dict(fs=xl), dict(fs=xo), dict(tp=other), dict(sp=zl), dict(grp=pair)]
    for where in near:
        pl.semaphore_signal(barrier, inc=1, device_id=where, device_id_type=MESH)

    pltpu.make_async_copy(stage, stage, load_sem.at[0]).wait()
    for n in others:
        loads[n].wait()

    sides = ((wq_ref, wk_ref), (wv_ref, wb_ref), (wc_ref, wi_ref), (woa_ref, woc_ref))
    for to in range(n_fs):
        lanes = slice(to * HD, (to + 1) * HD)
        for k, (left, right) in enumerate(sides):
            stage[to, k, :, 0:HD] = left[:, lanes]
            stage[to, k, :, HD:PAIR] = right[:, lanes]
    pl.semaphore_wait(barrier, len(near))

    pl.semaphore_signal(ready, inc=1, device_id=dict(sp=zr), device_id_type=MESH)

    def chunk_at(k, to):
        return out_at + n_fs * c + to if k == 3 else k

    def shard_copy(k, n, to, source):
        at = pl.ds(pl.multiple_of(z * zpart + source * part, part), part)
        return copy(stage.at[to, k], wall.at[chunk_at(k, to), at, :], send.at[0], w_recv.at[k], fs=to)

    for k in range(4):
        for n, to in ((2, xo), (0, xr), (1, xl)):
            shard_copy(k, n, to, x).start()
    here = pl.ds(pl.multiple_of(z * zpart + x * part, part), part)
    wall[0:3, here, :] = stage[x, 0:3]
    wall[out_at + me, here, :] = stage[x, 3]

    step_rows = min(rows, 32)
    for s in range(own_seqs):
        for r in range(0, rows, step_rows):
            wide = tok_ref[s, r : r + step_rows, :].astype(F32)
            scale = lax.rsqrt(jnp.mean(wide * wide, axis=-1, keepdims=True) + EPS)
            at = pl.multiple_of(c * own_rows + s * rows + r, step_rows)
            tokens[x, pl.ds(at, step_rows), :] = (wide * scale * norm_gain_ref[...]).astype(BF16)

    class RowGather:
        def __init__(self, ref, size, send, recv, j):
            self.ref, self.size, self.send, self.recv, self.j = ref, size, send, recv, j

        def one(self, n, i, part_of, **where):
            first, length = ((0, self.size), (0, self.size // 2), (self.size // 2, self.size // 2))[part_of]
            ref = self.ref(i, first, length)
            return copy(ref, ref, self.send, self.recv.at[self.j if n < 4 else 0, min(n, 4)], **where)

        def sent_as(self, n):
            i, part_of, where = (
                (x, 0, dict(fs=xr)),
                (x, 0, dict(fs=xl)),
                (xl, 1, dict(fs=xr)),
                (xr, 2, dict(fs=xl)),
                (x, 0, dict(tp=other)),
                (xl, 0, dict(tp=other)),
                (xr, 0, dict(tp=other)),
                (xo, 0, dict(tp=other)),
            )[n]
            return self.one(n, i, part_of, **where)

        def own(self):
            for n in (0, 1, 4):
                self.sent_as(n).start()

        def neighbours(self):
            self.one(0, xl, 0, fs=xr).wait_recv()
            self.sent_as(2).start()
            self.one(1, xr, 0, fs=xl).wait_recv()
            for n in (3, 5, 6):
                self.sent_as(n).start()

        def opposite(self):
            self.one(2, xo, 1, fs=xr).wait_recv()
            self.one(3, xo, 2, fs=xl).wait_recv()
            self.sent_as(7).start()

    def token_ref(core):
        def ref(i, first, length):
            return tokens.at[i, pl.ds(pl.multiple_of(core * own_rows + first, length), length), :]

        return ref

    token_gather = RowGather(token_ref(c), own_rows, send.at[1], t_recv, 0)

    lane = lax.broadcasted_iota(jnp.int32, lam_ref.shape, 1)
    chosen = jnp.sum(jnp.where(lane == x, lam_ref[...], 0.0), axis=-1, keepdims=True)
    lams[c] = jnp.broadcast_to(chosen, lams.shape[1:])
    lam_copy = copy(lams.at[c], lams.at[c], one_send.at[0], one_recv.at[0], tp=other)
    lam_copy.start()

    pieces_of = ((0, 0, 2), (0, 1, 2), (1, 0, 1), (2, 0, 2), (2, 1, 2), (3, 0, 2))

    def slice_ref(k, zb, side):
        kind, nth, count = pieces_of[k]
        length = zpart // count
        first = zb * zpart + (side if kind == 3 else nth) * length
        at = pl.ds(pl.multiple_of(first, length), length)
        if kind == 2:
            return wall.at[2 + side * (1 + me), at, :]
        return wall.at[(0, 1, 2, 1)[kind], at, (slice(0, PAIR), slice(0, HD), None, slice(HD, PAIR))[kind]]

    def ring_block(way, step):
        return lax.rem(z - step + 2 * n_sp, n_sp) if way == 0 else lax.rem(z + step, n_sp)

    def ring(way, step, k, ahead):
        ref = slice_ref(k, ring_block(way, step + ahead), odd)
        to = zr if way == 0 else zl
        return copy(ref, ref, send.at[2], ring_recv.at[way, step, k], sp=to)

    def pair_copy(way, step, k, side):
        ref = slice_ref(k, ring_block(way, step + 1), side)
        return copy(ref, ref, send.at[3], pair_recv.at[k // 5], grp=pair)

    def active(way, step, k):
        return step < half_ring - 1 or (step == half_ring - 1 and (k in (0, 1, 5)) == (way == 0))

    @pl.when(z != 0)
    def _():
        pl.semaphore_wait(ready, 1)

    for k in range(4):
        together(w_recv.at[k], 3 * shard_size).wait_recv()
        for slot, its in enumerate((0, 0, 1, 3, 3, 1)):
            if k == its:
                ring(0, 0, slot, 0).start()

                @pl.when(z != 0)
                def _():
                    ring(1, 0, slot, 0).start()

    token_gather.own()
    @pl.when(z == 0)
    def _():
        pl.semaphore_wait(ready, 1)
        for k in range(6):
            ring(1, 0, k, 0).start()

    def project(i, blocks, first=False):
        for k in range(2):
            lanes = slice(0, PAIR if k == 0 else HD)
            total = None if first else partial[k, i, :, lanes]
            for zb in blocks:
                at = pl.ds(pl.multiple_of(zb * zpart, zpart), zpart)
                add = jnp.dot(tokens[i, :, at], wall[k, at, lanes], preferred_element_type=F32)
                total = add if total is None else total + add
            partial[k, i, :, lanes] = total

    def blocks_of(steps):
        return [ring_block(way, step + 1) for step in steps for way in range(2)]

    late = half_ring - LATE
    for step in range(half_ring):
        for k in range(6):
            for way in range(2):
                if active(way, step, k):
                    ring(way, step, k, 1).wait_recv()
                    if active(way, step + 1, k):
                        ring(way, step + 1, k, 0).start()
                    if k >= 3:
                        pair_copy(way, step, k, odd).start()
            if k >= n_fs:
                continue
            if step > late:
                project(k, blocks_of((step - 1,)))
        if step == late - 2:
            token_gather.neighbours()
        if step == late - 1:
            token_gather.opposite()
        if step == late:
            together(t_recv.at[0, 4], n_fs * token_size).wait_recv()
            for i in range(n_fs):
                project(i, [z] + blocks_of(range(late)), first=True)
    last_block = [ring_block(0, half_ring)]

    pieces = wo_recv.shape[0]
    piece = width // pieces

    def w_out_ref(core, j):
        def ref(i, first, length):
            return wall.at[out_at + n_fs * core + i, pl.ds(j * piece + first, length), :]

        return ref

    w_out_gathers = [RowGather(w_out_ref(c, j), piece, send.at[5], wo_recv, j) for j in range(pieces)]

    lanes_x = pl.ds(pl.multiple_of(x * HD, HD), HD)
    low = lax.broadcasted_iota(jnp.int32, (2 * own_rows, HD), 1) < HALF

    def unit(raw, gain):
        wide = raw.astype(BF16).astype(F32)
        square = wide * wide
        first = jnp.sum(jnp.where(low, square, 0.0), axis=-1, keepdims=True)
        second = jnp.sum(jnp.where(low, 0.0, square), axis=-1, keepdims=True)
        scale = jnp.where(low, lax.rsqrt(first / HALF + EPS), lax.rsqrt(second / HALF + EPS))
        return wide * scale * gain

    for i in range(n_fs):
        project(i, last_block)
        both = partial[0, i]
        query = (unit(both[:, :HD], q_gain_ref[:, lanes_x]) * HALF**-0.5).astype(BF16)
        key = unit(both[:, HD:], k_gain_ref[:, lanes_x]).astype(BF16)
        value = partial[1, i, :, 0:HD].astype(BF16)
        for s in range(own_seqs):
            for core in range(2):
                src = slice(core * own_rows + s * rows, core * own_rows + (s + 1) * rows)
                dst = slice(core * rows, (core + 1) * rows)
                qkv[own_seqs * i + s, dst, 0:HD] = query[src]
                qkv[own_seqs * i + s, dst, HD:PAIR] = key[src]
                qkv[own_seqs * i + s, dst, PAIR:] = value[src]

    def owner(zb):
        return lax.rem(lax.rem(zb, 2) + zb // 2, 2)

    def own_block(i):
        return 2 * i + lax.rem(i + c, 2)

    def other_block(i):
        return 2 * i + lax.rem(i + other, 2)

    offsets = [n_seq // 2]
    for d in range(n_seq // 2 - 1, 0, -1):
        offsets += [d, n_seq - d]
    my_owner = owner(z)

    last = len(offsets)

    def qkv_copy(n, offset):
        s = lax.rem(z // 2 + offset, n_seq)
        return copy(qkv.at[s], heads.at[z], send.at[4 if n < last else 9], a_recv.at[z // 2], sp=2 * s + c, tp=my_owner)

    for n, offset in enumerate(offsets):
        qkv_copy(n, offset).start()
    home = (c == lax.rem(z, 2)) & (my_owner == c)
    away = (c != lax.rem(z, 2)) | (my_owner != c)

    @pl.when(away)
    def _():
        qkv_copy(last, 0).start()

    @pl.when(home)
    def _():
        heads[z] = qkv[z // 2]

    together(pair_recv.at[0], (n_sp - 1) * slice_size).wait_recv()
    together(pair_recv.at[1], (n_sp - 1) * slice_size // 4).wait_recv()
    for gather in w_out_gathers:
        gather.own()

    @pl.loop(0, n_fs)
    def _(i):
        both = jnp.dot(tokens[i], wall[2], preferred_element_type=F32).astype(BF16)
        both = both.astype(F32)
        gate_b[i] = jnp.dot(tokens[i], wall[1, :, HD:PAIR], preferred_element_type=F32).astype(BF16)
        product = (both[:, :HD] * both[:, HD:]).astype(BF16).astype(F32)
        for s in range(own_seqs):
            for core in range(2):
                src = slice(core * own_rows + s * rows, core * own_rows + (s + 1) * rows)
                shaped[own_seqs * i + s, TAIL + core * rows : TAIL + (core + 1) * rows, :] = product[src]

    tail_copy = copy(
        shaped.at[:, block : block + TAIL, :],
        shaped.at[:, 0:TAIL, :],
        one_send.at[1],
        one_recv.at[1],
        sp=zr,
    )
    tail_copy.start()
    for gather in w_out_gathers:
        gather.neighbours()

    def kv_copy(i, zb):
        ref = heads.at[zb, :, HD:]
        return copy(ref, ref, send.at[7], kv_recv.at[0], tp=other)

    for i in range(n_seq):
        zb = own_block(i)

        @pl.when((zb != z) | (c != lax.rem(z, 2)))
        def _():
            copy(qkv.at[0], heads.at[zb], send.at[4], a_recv.at[i], sp=zb, tp=c).wait_recv()

        kv_copy(i, zb).start()
    tail_copy.wait_recv()

    @pl.when(z == 0)
    def _():
        shaped[:, 0:TAIL, :] = jnp.zeros((n_seq, TAIL, HD), F32)

    taps = [taps_ref[i : i + 1, lanes_x] for i in range(3)]

    @pl.loop(0, n_fs)
    def _(i):
        for s in range(own_seqs):
            seq = own_seqs * i + s
            total = taps[0] * shaped[seq, TAIL - 2 : TAIL - 2 + block, :]
            total = total + taps[1] * shaped[seq, TAIL - 1 : TAIL - 1 + block, :]
            total = total + taps[2] * shaped[seq, TAIL : TAIL + block, :]
            for core in range(2):
                gate = gate_b[i, core * own_rows + s * rows : core * own_rows + (s + 1) * rows, :]
                gated = gate.astype(F32) * total[core * rows : (core + 1) * rows]
                conv[2 * i + core, s * rows : (s + 1) * rows, :] = gated.astype(BF16)

    def conv_copy(n, to, core):
        return copy(conv.at[2 * to + core], conv_all.at[me], send.at[6], c_recv.at[0], fs=to, tp=core)

    conv_to = [(xo, c), (xo, other), (xr, c), (xr, other), (xl, c), (xl, other), (x, other)]
    for n, (to, core) in enumerate(conv_to):
        conv_copy(n, to, core).start()
    conv_all[me] = conv[2 * x + c]


    for gather in w_out_gathers[:-1]:
        gather.opposite()
    lam_copy.wait_recv()
    together(kv_recv.at[0], n_seq * kv_size).wait_recv()

    seq, mine = z // 2, lax.rem(z, 2)
    head = n_fs * mine + x
    seq_x, seq_row = seq // own_seqs, pl.ds(pl.multiple_of(lax.rem(seq, own_seqs) * rows, rows), rows)
    lane = lax.broadcasted_iota(jnp.int32, (block, HD), 1)
    key_at = lax.broadcasted_iota(jnp.int32, (2 * block, keys), 1)
    row_at = lax.rem(lax.broadcasted_iota(jnp.int32, (2 * block, keys), 0), block)

    def out_copy(i, zb, core):
        return copy(
            attn.at[i, core * rows : (core + 1) * rows, :],
            attn_all.at[head, seq_row, :],
            send.at[8],
            o_recv.at[head // 2],
            fs=seq_x,
            sp=zb,
            tp=core,
        )

    def is_self(zb, core):
        return (seq_x == x) & (zb == z) & (c == core)

    def not_self(zb, core):
        return (seq_x != x) | (zb != z) | (c != core)

    def scored(i, first):
        zb = own_block(i)
        query = heads[zb, :, 0:HD].astype(F32)
        query = jnp.concatenate(
            [jnp.where(lane < HALF, query, 0.0), jnp.where(lane < HALF, 0.0, query)], axis=0
        ).astype(BF16)
        top = None
        for j in range(i + 1):
            key = heads[2 * j : 2 * j + 2, :, HD:PAIR].reshape(keys, HD)
            s = lax.dot_general(query, key, (((1,), (1,)), ((), ())), preferred_element_type=F32)
            if j == i:
                s = jnp.where(key_at <= row_at + block * lax.rem(i + c, 2), s, NEG)
            score[:, first + j * keys : first + (j + 1) * keys] = s
            top = folded(jnp.maximum, s, top)
        return jnp.max(top, axis=-1, keepdims=True)

    def folded(op, s, start):
        for n in range(0, keys, min(HD, keys)):
            piece = s[:, n : n + min(HD, keys)]
            start = piece if start is None else op(start, piece)
        return start

    def weighted(i, first, top):
        total, summed = None, None
        for j in range(i + 1):
            weight = jnp.exp(score[:, first + j * keys : first + (j + 1) * keys] - top)
            value = heads[2 * j : 2 * j + 2, :, PAIR:].reshape(keys, HD)
            add = jnp.dot(weight.astype(BF16), value, preferred_element_type=F32)
            total = folded(jnp.add, weight, total)
            summed = add if summed is None else summed + add
        return summed, jnp.sum(total, axis=-1, keepdims=True)

    def finished(i, summed, total):
        maps = summed / total
        differ = maps[:block] - lams[mine][0:1, :] * maps[block:]
        scale = lax.rsqrt(jnp.mean(differ * differ, axis=-1, keepdims=True) + EPS)
        attn[i] = (differ * scale * head_gain_ref[...] * OUT_SCALE).astype(BF16)

    def deliver(i):
        zb = own_block(i)
        for core in range(2):

            @pl.when(not_self(zb, core))
            def _():
                out_copy(i, zb, core).start()

            @pl.when(is_self(zb, core))
            def _():
                attn_all[head, seq_row, :] = attn[i, core * rows : (core + 1) * rows, :]

    side = jnp.minimum(seq, n_seq - 1 - seq)

    @pl.loop(0, n_seq // 2)
    def _(turn):
        late_turn = turn // 2
        inner = side // 2
        first = n_seq // 2 - 1 - side
        now = (1 - late_turn) * (first + lax.rem(turn, 2) * (1 - 2 * lax.rem(first, 2))) + late_turn * (
            inner * turn + (1 - inner) * (n_seq // 2 - 1 - turn)
        )
        for p in range(n_seq // 2):

            @pl.when(now == p)
            def _():
                both = ((n_seq - 1 - p, 0), (p, n_sp * block))
                tops = [scored(i, first) for i, first in both]
                sums = [weighted(i, first, top) for (i, first), top in zip(both, tops)]
                for (i, _), (summed, total) in zip(both, sums):
                    finished(i, summed, total)
                for i, _ in both:
                    deliver(i)

    w_out_gathers[-1].opposite()
    together(wo_recv.at[0, 4], n_fs * width * 2 * PAIR).wait_recv()
    together(c_recv.at[0], len(conv_to) * conv_size).wait_recv()
    columns = min(width, 256)

    def projected(features, lanes, at, h):
        weight = jnp.concatenate([wall[out_at + h, at, lanes], wall[out_at + h + 1, at, lanes]], axis=1)
        pair_of = jnp.concatenate([features[h], features[h + 1]], axis=1)
        return lax.dot_general(pair_of, weight, (((1,), (1,)), ((), ())), preferred_element_type=F32)

    def column(n):
        return pl.ds(pl.multiple_of(n * columns, columns), columns)

    @pl.loop(0, width // columns)
    def _(n):
        at = column(n)
        mixed[:, at] = sum(projected(conv_all, slice(HD, PAIR), at, h) for h in range(0, 2 * n_fs, 2))

    kept = (seq_x == x) & (my_owner == c)
    sent_all = (seq_x != x) | (my_owner != c)
    for h in range(0, 2 * n_fs, 2):
        here_too = kept & (head // 2 == h // 2)
        not_here = sent_all | (head // 2 != h // 2)

        @pl.when(here_too)
        def _():
            together(o_recv.at[h // 2], (2 * own_seqs - 1) * out_size).wait_recv()

        @pl.when(not_here)
        def _():
            together(o_recv.at[h // 2], 2 * own_seqs * out_size).wait_recv()

        if h < 2 * n_fs - 2:

            @pl.loop(0, width // columns)
            def _(n):
                at = column(n)
                mixed[:, at] += projected(attn_all, slice(0, HD), at, h)

    @pl.loop(0, width // columns)
    def _(n):
        at = column(n)
        total = mixed[:, at] + projected(attn_all, slice(0, HD), at, 2 * n_fs - 2)
        for s in range(own_seqs):
            out_ref[s, :, at] = total[s * rows : (s + 1) * rows].astype(BF16)

    together(send.at[0], 12 * shard_size).wait_send()
    together(send.at[1], 7 * token_size).wait_send()
    together(send.at[2], (n_sp - 1) * slice_size * 11 // 4).wait_send()
    together(send.at[3], (n_sp - 1) * slice_size * 5 // 4).wait_send()
    together(send.at[4], last * block * 6 * HD).wait_send()
    together(send.at[5], 7 * width * 2 * PAIR).wait_send()
    together(send.at[6], len(conv_to) * conv_size).wait_send()
    together(send.at[7], n_seq * kv_size).wait_send()
    lam_copy.wait_send()
    tail_copy.wait_send()

    @pl.when(away)
    def _():
        qkv_copy(last, 0).wait_send()

    @pl.when(kept)
    def _():
        together(send.at[8], (2 * n_seq - 1) * out_size).wait_send()

    @pl.when(sent_all)
    def _():
        together(send.at[8], 2 * n_seq * out_size).wait_send()


def on_device(n_grp, n_sp, n_fs, *args):
    tokens, norm_gain, wq, wk, wv, q_gain, k_gain, lam, head_gain, wb, wc, wi, taps, woa, woc = args
    own_seqs, rows, width = tokens.shape
    n_seq, block, n_head = own_seqs * n_fs, 2 * rows, 2 * n_fs
    assert n_grp % 2 == 0 and n_sp == 2 * n_seq and n_fs == 4 and own_seqs == 2
    half_ring = n_sp // 2
    row = lambda v: v.reshape(1, -1)
    ins = (
        tokens, row(norm_gain), wq, wk, wv, row(q_gain), row(k_gain), row(lam), row(head_gain),
        wb, wc, wi, taps, woa.T, woc.T,
    )
    dma = pltpu.SemaphoreType.DMA
    vmem = pl.BlockSpec(memory_space=pltpu.VMEM)
    call = pl.pallas_call(
        functools.partial(kernel, n_grp, n_sp, n_fs),
        out_shape=jax.ShapeDtypeStruct(tokens.shape, BF16),
        in_specs=[pl.BlockSpec(memory_space=pltpu.HBM)] * 15,
        out_specs=vmem,
        scratch_shapes=[pltpu.VMEM(a.shape, a.dtype) for a in ins]
        + [
            pltpu.VMEM((n_fs, 2 * own_seqs * rows, width), BF16),
            pltpu.VMEM((n_fs, 4, wq.shape[0], PAIR), BF16),
            pltpu.VMEM((3 + n_head, width, PAIR), BF16),
            pltpu.VMEM((2, n_fs, 2 * own_seqs * rows, PAIR), F32),
            pltpu.VMEM((n_seq, block, 3 * HD), BF16),
            pltpu.VMEM((n_fs, 2 * own_seqs * rows, HD), BF16),
            pltpu.VMEM((n_sp, block, 3 * HD), BF16),
            pltpu.VMEM((2 * block, n_sp * block * 3 // 2), F32),
            pltpu.VMEM((n_seq, block, HD), BF16),
            pltpu.VMEM((n_head, own_seqs * rows, HD), BF16),
            pltpu.VMEM((n_seq, TAIL + block, HD), F32),
            pltpu.VMEM((n_head, own_seqs * rows, HD), BF16),
            pltpu.VMEM((n_head, own_seqs * rows, HD), BF16),
            pltpu.VMEM((2, 8, HD), F32),
            pltpu.VMEM((own_seqs * rows, width), F32),
            dma((10,)),
            dma((4,)),
            dma((1, 5)),
            dma((2, half_ring, 6)),
            dma((2,)),
            pltpu.SemaphoreType.REGULAR,
            dma((n_seq,)),
            dma((1,)),
            dma((n_fs,)),
            dma((1,)),
            dma((4, 5)),
            dma((2,)),
            dma((2,)),
            dma((8,)),
        ],
        compiler_params=pltpu.CompilerParams(
            collective_id=0, has_side_effects=True, vmem_limit_bytes=32 * 1024 * 1024
        ),
    )
    return call(*[pltpu.with_memory_space_constraint(a, pltpu.HBM) for a in ins])


def solution(mesh):
    placed = (
        P(("grp", "fs"), ("sp", "tp"), None),
        P(),
        P(("sp", "fs"), "tp"),
        P(("sp", "fs"), "tp"),
        P(("sp", "fs"), "tp"),
        P("tp"),
        P("tp"),
        P("tp"),
        P(),
        P(("sp", "fs"), "tp"),
        P(("sp", "fs"), "tp"),
        P(("sp", "fs"), "tp"),
        P(None, "tp"),
        P("tp", ("sp", "fs")),
        P("tp", ("sp", "fs")),
    )
    return jax.shard_map(
        functools.partial(on_device, mesh.shape["grp"], mesh.shape["sp"], mesh.shape["fs"]),
        mesh=mesh,
        in_specs=placed,
        out_specs=P(("grp", "fs"), ("sp", "tp"), None),
        check_vma=False,
    )
```

```python
import functools

import jax
import jax.numpy as jnp
from jax import lax
from jax.experimental import pallas as pl
from jax.experimental.pallas import tpu as pltpu
from jax.sharding import PartitionSpec as P

EPS = 1e-06
NEG = -1e30
OUT_SCALE = 0.8
HD = 128
HALF = HD // 2
PAIR = 2 * HD
TAIL = 8
F32 = jnp.float32
BF16 = jnp.bfloat16
MESH = pl.DeviceIdType.MESH


def kernel(
    n_grp,
    n_sp,
    n_fs,
    *refs,
):
    (tok_ref, norm_gain_ref, wq_ref, wk_ref, wv_ref, q_gain_ref, k_gain_ref, lam_ref, head_gain_ref, wb_ref, wc_ref, wi_ref, taps_ref, woa_ref, woc_ref) = refs[16:31]
    (
    out_ref,
    tokens,
    stage,
    wall,
    partial,
    qkv,
    gate_b,
    heads,
    score,
    attn,
    attn_all,
    shaped,
    conv,
    conv_all,
    lams,
    mixed,
    send,
    w_recv,
    t_recv,
    ring_recv,
    pair_recv,
    ready,
    a_recv,
    kv_recv,
    o_recv,
    c_recv,
    wo_recv,
    one_send,
    one_recv,
    load_sem,
    ) = (refs[15], *refs[31:])
    weights, others = (2, 3, 4, 9, 10, 11, 13, 14), (0, 1, 5, 6, 7, 8, 12)
    load_at = {n: 0 for n in weights} | {n: 1 + i for i, n in enumerate(others)}
    loads = [pltpu.make_async_copy(refs[n], refs[16 + n], load_sem.at[load_at[n]]) for n in range(15)]
    for n in weights + others:
        loads[n].start()
    g = lax.axis_index("grp")
    z, x, c = lax.axis_index("sp"), lax.axis_index("fs"), lax.axis_index("tp")
    own_seqs, rows, width = tok_ref.shape
    own_rows = own_seqs * rows
    block = 2 * rows
    keys = 2 * block
    part = wq_ref.shape[0]
    zpart = n_fs * part
    n_seq = own_seqs * n_fs
    half_ring = n_sp // 2
    xr, xl, xo = lax.rem(x + 1, n_fs), lax.rem(x + n_fs - 1, n_fs), lax.rem(x + 2, n_fs)
    zr, zl = lax.rem(z + 1, n_sp), lax.rem(z + n_sp - 1, n_sp)
    other = 1 - c
    me = n_fs * c + x
    odd = lax.rem(g, 2)
    pair = g + 1 - 2 * odd
    out_at = 3

    def copy(src, dst, send, recv, **where):
        return pltpu.make_async_remote_copy(
            src_ref=src,
            dst_ref=dst,
            send_sem=send,
            recv_sem=recv,
            device_id=where,
            device_id_type=MESH,
        )

    def together(sem, size):
        lines = size // (2 * PAIR)
        for most in range(1, wall.shape[0] + 1):
            if lines % most == 0 and lines // most <= width and lines // most % 16 == 0:
                ref = wall.at[0:most, 0 : lines // most, :]
                return copy(ref, ref, sem, sem, tp=other)
        raise ValueError(size)

    shard_size, slice_size = part * 2 * PAIR, zpart * 2 * PAIR
    token_size, conv_size = own_rows * width * 2, own_rows * HD * 2
    out_size, kv_size = rows * HD * 2, block * 2 * PAIR

    barrier = pltpu.get_barrier_semaphore()
    near = [dict(fs=xr), dict(fs=xl), dict(fs=xo), dict(tp=other), dict(sp=zl), dict(grp=pair)]
    for where in near:
        pl.semaphore_signal(barrier, inc=1, device_id=where, device_id_type=MESH)

    pltpu.make_async_copy(stage, stage, load_sem.at[0]).wait()
    for n in others:
        loads[n].wait()

    sides = ((wq_ref, wk_ref), (wv_ref, wb_ref), (wc_ref, wi_ref), (woa_ref, woc_ref))
    for to in range(n_fs):
        lanes = slice(to * HD, (to + 1) * HD)
        for k, (left, right) in enumerate(sides):
            stage[to, k, :, 0:HD] = left[:, lanes]
            stage[to, k, :, HD:PAIR] = right[:, lanes]
    pl.semaphore_wait(barrier, len(near))

    pl.semaphore_signal(ready, inc=1, device_id=dict(sp=zr), device_id_type=MESH)

    def chunk_at(k, to):
        return out_at + n_fs * c + to if k == 3 else k

    def shard_copy(k, n, to, source):
        at = pl.ds(pl.multiple_of(z * zpart + source * part, part), part)
        return copy(stage.at[to, k], wall.at[chunk_at(k, to), at, :], send.at[0], w_recv.at[k], fs=to)

    for k in range(4):
        for n, to in ((2, xo), (0, xr), (1, xl)):
            shard_copy(k, n, to, x).start()
    here = pl.ds(pl.multiple_of(z * zpart + x * part, part), part)
    wall[0:3, here, :] = stage[x, 0:3]
    wall[out_at + me, here, :] = stage[x, 3]

    step_rows = min(rows, 32)
    for s in range(own_seqs):
        for r in range(0, rows, step_rows):
            wide = tok_ref[s, r : r + step_rows, :].astype(F32)
            scale = lax.rsqrt(jnp.mean(wide * wide, axis=-1, keepdims=True) + EPS)
            at = pl.multiple_of(c * own_rows + s * rows + r, step_rows)
            tokens[x, pl.ds(at, step_rows), :] = (wide * scale * norm_gain_ref[...]).astype(BF16)

    class RowGather:
        def __init__(self, ref, size, send, recv, j):
            self.ref, self.size, self.send, self.recv, self.j = ref, size, send, recv, j

        def one(self, n, i, part_of, **where):
            first, length = ((0, self.size), (0, self.size // 2), (self.size // 2, self.size // 2))[part_of]
            ref = self.ref(i, first, length)
            return copy(ref, ref, self.send, self.recv.at[self.j if n < 4 else 0, min(n, 4)], **where)

        def sent_as(self, n):
            i, part_of, where = (
                (x, 0, dict(fs=xr)),
                (x, 0, dict(fs=xl)),
                (xl, 1, dict(fs=xr)),
                (xr, 2, dict(fs=xl)),
                (x, 0, dict(tp=other)),
                (xl, 0, dict(tp=other)),
                (xr, 0, dict(tp=other)),
                (xo, 0, dict(tp=other)),
            )[n]
            return self.one(n, i, part_of, **where)

        def own(self):
            for n in (0, 1, 4):
                self.sent_as(n).start()

        def neighbours(self):
            self.one(0, xl, 0, fs=xr).wait_recv()
            self.sent_as(2).start()
            self.one(1, xr, 0, fs=xl).wait_recv()
            for n in (3, 5, 6):
                self.sent_as(n).start()

        def opposite(self):
            self.one(2, xo, 1, fs=xr).wait_recv()
            self.one(3, xo, 2, fs=xl).wait_recv()
            self.sent_as(7).start()

    def token_ref(core):
        def ref(i, first, length):
            return tokens.at[i, pl.ds(pl.multiple_of(core * own_rows + first, length), length), :]

        return ref

    token_gather = RowGather(token_ref(c), own_rows, send.at[1], t_recv, 0)

    lane = lax.broadcasted_iota(jnp.int32, lam_ref.shape, 1)
    chosen = jnp.sum(jnp.where(lane == x, lam_ref[...], 0.0), axis=-1, keepdims=True)
    lams[c] = jnp.broadcast_to(chosen, lams.shape[1:])
    lam_copy = copy(lams.at[c], lams.at[c], one_send.at[0], one_recv.at[0], tp=other)
    lam_copy.start()

    pieces_of = ((0, 0), (1, 0), (2, 0), (2, 1), (3, 0))

    def slice_ref(k, zb, side):
        kind, nth = pieces_of[k]
        length = zpart // 2
        at = pl.ds(pl.multiple_of(zb * zpart + (nth if kind == 2 else side) * length, length), length)
        if kind == 2:
            return wall.at[2 + side * (1 + me), at, :]
        return wall.at[(0, 1, 2, 1)[kind], at, (slice(0, PAIR), slice(0, HD), None, slice(HD, PAIR))[kind]]

    def ring_block(way, step):
        return lax.rem(z - step + 2 * n_sp, n_sp) if way == 0 else lax.rem(z + step, n_sp)

    def ring(way, step, k, ahead):
        ref = slice_ref(k, ring_block(way, step + ahead), odd)
        to = zr if way == 0 else zl
        return copy(ref, ref, send.at[2], ring_recv.at[way, step, k], sp=to)

    soon = half_ring - 3

    def pair_copy(way, step, k, side):
        ref = slice_ref(k, ring_block(way, step + 1), side)
        recv = pair_recv.at[6 if k == 4 else 0 if step < soon else 1]
        return copy(ref, ref, send.at[3], recv, grp=pair)

    pieces = wo_recv.shape[0]
    piece = width // pieces

    def pair_piece(j, side):
        ref = wall.at[2 + side * (1 + me), pl.ds(j * piece, piece), :]
        return copy(ref, ref, send.at[3], pair_recv.at[2 + j], grp=pair)

    def active(way, step, k):
        return step < half_ring - 1 or (step == half_ring - 1 and (k in (0, 2)) == (way == 0))

    @pl.when(z != 0)
    def _():
        pl.semaphore_wait(ready, 1)

    for k in range(4):
        together(w_recv.at[k], 3 * shard_size).wait_recv()
        for slot, its in enumerate((0, 1, 3, 3, 1)):
            if k == its:
                ring(0, 0, slot, 0).start()

                @pl.when(z != 0)
                def _():
                    ring(1, 0, slot, 0).start()

    token_gather.own()
    @pl.when(z == 0)
    def _():
        pl.semaphore_wait(ready, 1)
        for k in range(5):
            ring(1, 0, k, 0).start()

    def project(i, blocks, first=False):
        for k in range(2):
            lanes = slice(0, PAIR if k == 0 else HD)
            total = None if first else partial[k, i, :, lanes]
            for zb in blocks:
                at = pl.ds(pl.multiple_of(zb * zpart, zpart), zpart)
                add = jnp.dot(tokens[i, :, at], wall[k, at, lanes], preferred_element_type=F32)
                total = add if total is None else total + add
            partial[k, i, :, lanes] = total

    def blocks_of(steps):
        return [ring_block(way, step + 1) for step in steps for way in range(2)]

    for step in range(half_ring):
        for k in range(5):
            for way in range(2):
                if active(way, step, k):
                    ring(way, step, k, 1).wait_recv()
                    if active(way, step + 1, k):
                        ring(way, step + 1, k, 0).start()
                    if k < 2:
                        pair_copy(way, step, k, odd).start()
        if step == half_ring // 2:
            token_gather.neighbours()
        if step == half_ring - 2:
            token_gather.opposite()
    together(pair_recv.at[0], 2 * soon * slice_size * 3 // 4).wait_recv()
    for j in range(pieces):
        pair_piece(j, odd).start()
    for step in range(half_ring):
        for way in range(2):
            if active(way, step, 4):
                pair_copy(way, step, 4, odd).start()
    together(t_recv.at[0, 4], n_fs * token_size).wait_recv()
    for i in range(n_fs):
        project(i, [z] + blocks_of(range(soon)), first=True)
    together(pair_recv.at[1], (n_sp - 1 - 2 * soon) * slice_size * 3 // 4).wait_recv()
    last_blocks = blocks_of(range(soon, half_ring - 1)) + [ring_block(0, half_ring)]

    def w_out_ref(core, j):
        def ref(i, first, length):
            return wall.at[out_at + n_fs * core + i, pl.ds(j * piece + first, length), :]

        return ref

    w_out_gathers = [RowGather(w_out_ref(c, j), piece, send.at[5], wo_recv, j) for j in range(pieces)]

    lanes_x = pl.ds(pl.multiple_of(x * HD, HD), HD)
    low = lax.broadcasted_iota(jnp.int32, (2 * own_rows, HD), 1) < HALF

    def unit(raw, gain):
        wide = raw.astype(BF16).astype(F32)
        square = wide * wide
        first = jnp.sum(jnp.where(low, square, 0.0), axis=-1, keepdims=True)
        second = jnp.sum(jnp.where(low, 0.0, square), axis=-1, keepdims=True)
        scale = jnp.where(low, lax.rsqrt(first / HALF + EPS), lax.rsqrt(second / HALF + EPS))
        return wide * scale * gain

    for i in range(n_fs):
        project(i, last_blocks)
        both = partial[0, i]
        query = (unit(both[:, :HD], q_gain_ref[:, lanes_x]) * HALF**-0.5).astype(BF16)
        key = unit(both[:, HD:], k_gain_ref[:, lanes_x]).astype(BF16)
        value = partial[1, i, :, 0:HD].astype(BF16)
        for s in range(own_seqs):
            for core in range(2):
                src = slice(core * own_rows + s * rows, core * own_rows + (s + 1) * rows)
                dst = slice(core * rows, (core + 1) * rows)
                qkv[own_seqs * i + s, dst, 0:HD] = query[src]
                qkv[own_seqs * i + s, dst, HD:PAIR] = key[src]
                qkv[own_seqs * i + s, dst, PAIR:] = value[src]

    def owner(zb):
        return lax.rem(lax.rem(zb, 2) + zb // 2, 2)

    def own_block(i):
        return 2 * i + lax.rem(i + c, 2)

    def other_block(i):
        return 2 * i + lax.rem(i + other, 2)

    offsets = [n_seq // 2]
    for d in range(n_seq // 2 - 1, 0, -1):
        offsets += [d, n_seq - d]
    my_owner = owner(z)

    last = len(offsets)

    def qkv_copy(n, offset):
        s = lax.rem(z // 2 + offset, n_seq)
        return copy(qkv.at[s], heads.at[z], send.at[4 if n < last else 9], a_recv.at[z // 2], sp=2 * s + c, tp=my_owner)

    for n, offset in enumerate(offsets):
        qkv_copy(n, offset).start()
    home = (c == lax.rem(z, 2)) & (my_owner == c)
    away = (c != lax.rem(z, 2)) | (my_owner != c)

    @pl.when(away)
    def _():
        qkv_copy(last, 0).start()

    @pl.when(home)
    def _():
        heads[z] = qkv[z // 2]

    for j, gather in enumerate(w_out_gathers):
        together(pair_recv.at[2 + j], piece * 2 * PAIR).wait_recv()
        gather.own()
    together(pair_recv.at[6], (n_sp - 1) * slice_size // 4).wait_recv()

    @pl.loop(0, n_fs)
    def _(i):
        both = jnp.dot(tokens[i], wall[2], preferred_element_type=F32).astype(BF16)
        both = both.astype(F32)
        gate_b[i] = jnp.dot(tokens[i], wall[1, :, HD:PAIR], preferred_element_type=F32).astype(BF16)
        product = (both[:, :HD] * both[:, HD:]).astype(BF16).astype(F32)
        for s in range(own_seqs):
            for core in range(2):
                src = slice(core * own_rows + s * rows, core * own_rows + (s + 1) * rows)
                shaped[own_seqs * i + s, TAIL + core * rows : TAIL + (core + 1) * rows, :] = product[src]

    tail_copy = copy(
        shaped.at[:, block : block + TAIL, :],
        shaped.at[:, 0:TAIL, :],
        one_send.at[1],
        one_recv.at[1],
        sp=zr,
    )
    tail_copy.start()
    for gather in w_out_gathers:
        gather.neighbours()

    def kv_copy(i, zb):
        ref = heads.at[zb, :, HD:]
        return copy(ref, ref, send.at[7], kv_recv.at[0], tp=other)

    for i in range(n_seq):
        zb = own_block(i)

        @pl.when((zb != z) | (c != lax.rem(z, 2)))
        def _():
            copy(qkv.at[0], heads.at[zb], send.at[4], a_recv.at[i], sp=zb, tp=c).wait_recv()

        kv_copy(i, zb).start()
    tail_copy.wait_recv()

    @pl.when(z == 0)
    def _():
        shaped[:, 0:TAIL, :] = jnp.zeros((n_seq, TAIL, HD), F32)

    taps = [taps_ref[i : i + 1, lanes_x] for i in range(3)]

    @pl.loop(0, n_fs)
    def _(i):
        for s in range(own_seqs):
            seq = own_seqs * i + s
            total = taps[0] * shaped[seq, TAIL - 2 : TAIL - 2 + block, :]
            total = total + taps[1] * shaped[seq, TAIL - 1 : TAIL - 1 + block, :]
            total = total + taps[2] * shaped[seq, TAIL : TAIL + block, :]
            for core in range(2):
                gate = gate_b[i, core * own_rows + s * rows : core * own_rows + (s + 1) * rows, :]
                gated = gate.astype(F32) * total[core * rows : (core + 1) * rows]
                conv[2 * i + core, s * rows : (s + 1) * rows, :] = gated.astype(BF16)

    def conv_copy(n, to, core):
        return copy(conv.at[2 * to + core], conv_all.at[me], send.at[6], c_recv.at[0], fs=to, tp=core)

    conv_to = [(xo, c), (xo, other), (xr, c), (xr, other), (xl, c), (xl, other), (x, other)]
    for n, (to, core) in enumerate(conv_to):
        conv_copy(n, to, core).start()
    conv_all[me] = conv[2 * x + c]


    for gather in w_out_gathers[:-1]:
        gather.opposite()
    lam_copy.wait_recv()
    together(kv_recv.at[0], n_seq * kv_size).wait_recv()

    seq, mine = z // 2, lax.rem(z, 2)
    head = n_fs * mine + x
    seq_x, seq_row = seq // own_seqs, pl.ds(pl.multiple_of(lax.rem(seq, own_seqs) * rows, rows), rows)
    lane = lax.broadcasted_iota(jnp.int32, (block, HD), 1)
    key_at = lax.broadcasted_iota(jnp.int32, (2 * block, keys), 1)
    row_at = lax.rem(lax.broadcasted_iota(jnp.int32, (2 * block, keys), 0), block)

    def out_copy(i, zb, core):
        return copy(
            attn.at[i, core * rows : (core + 1) * rows, :],
            attn_all.at[head, seq_row, :],
            send.at[8],
            o_recv.at[head // 2],
            fs=seq_x,
            sp=zb,
            tp=core,
        )

    def is_self(zb, core):
        return (seq_x == x) & (zb == z) & (c == core)

    def not_self(zb, core):
        return (seq_x != x) | (zb != z) | (c != core)

    def scored(i, first):
        zb = own_block(i)
        query = heads[zb, :, 0:HD].astype(F32)
        query = jnp.concatenate(
            [jnp.where(lane < HALF, query, 0.0), jnp.where(lane < HALF, 0.0, query)], axis=0
        ).astype(BF16)
        top = None
        for j in range(i + 1):
            key = heads[2 * j : 2 * j + 2, :, HD:PAIR].reshape(keys, HD)
            s = lax.dot_general(query, key, (((1,), (1,)), ((), ())), preferred_element_type=F32)
            if j == i:
                s = jnp.where(key_at <= row_at + block * lax.rem(i + c, 2), s, NEG)
            score[:, first + j * keys : first + (j + 1) * keys] = s
            top = folded(jnp.maximum, s, top)
        return jnp.max(top, axis=-1, keepdims=True)

    def folded(op, s, start):
        for n in range(0, keys, min(HD, keys)):
            piece = s[:, n : n + min(HD, keys)]
            start = piece if start is None else op(start, piece)
        return start

    def weighted(i, first, top):
        total, summed = None, None
        for j in range(i + 1):
            weight = jnp.exp(score[:, first + j * keys : first + (j + 1) * keys] - top)
            value = heads[2 * j : 2 * j + 2, :, PAIR:].reshape(keys, HD)
            add = jnp.dot(weight.astype(BF16), value, preferred_element_type=F32)
            total = folded(jnp.add, weight, total)
            summed = add if summed is None else summed + add
        return summed, jnp.sum(total, axis=-1, keepdims=True)

    def finished(i, summed, total):
        maps = summed / total
        differ = maps[:block] - lams[mine][0:1, :] * maps[block:]
        scale = lax.rsqrt(jnp.mean(differ * differ, axis=-1, keepdims=True) + EPS)
        attn[i] = (differ * scale * head_gain_ref[...] * OUT_SCALE).astype(BF16)

    def deliver(i):
        zb = own_block(i)
        for core in range(2):

            @pl.when(not_self(zb, core))
            def _():
                out_copy(i, zb, core).start()

            @pl.when(is_self(zb, core))
            def _():
                attn_all[head, seq_row, :] = attn[i, core * rows : (core + 1) * rows, :]

    side = jnp.minimum(seq, n_seq - 1 - seq)

    @pl.loop(0, n_seq // 2)
    def _(turn):
        late_turn = turn // 2
        inner = side // 2
        first = n_seq // 2 - 1 - side
        now = (1 - late_turn) * (first + lax.rem(turn, 2) * (1 - 2 * lax.rem(first, 2))) + late_turn * (
            inner * turn + (1 - inner) * (n_seq // 2 - 1 - turn)
        )
        for p in range(n_seq // 2):

            @pl.when(now == p)
            def _():
                both = ((n_seq - 1 - p, 0), (p, n_sp * block))
                tops = [scored(i, first) for i, first in both]
                sums = [weighted(i, first, top) for (i, first), top in zip(both, tops)]
                for (i, _), (summed, total) in zip(both, sums):
                    finished(i, summed, total)
                for i, _ in both:
                    deliver(i)

    w_out_gathers[-1].opposite()
    together(wo_recv.at[0, 4], n_fs * width * 2 * PAIR).wait_recv()
    together(c_recv.at[0], len(conv_to) * conv_size).wait_recv()
    columns = min(width, 256)

    def projected(features, lanes, at, h):
        weight = jnp.concatenate([wall[out_at + h, at, lanes], wall[out_at + h + 1, at, lanes]], axis=1)
        pair_of = jnp.concatenate([features[h], features[h + 1]], axis=1)
        return lax.dot_general(pair_of, weight, (((1,), (1,)), ((), ())), preferred_element_type=F32)

    def column(n):
        return pl.ds(pl.multiple_of(n * columns, columns), columns)

    @pl.loop(0, width // columns)
    def _(n):
        at = column(n)
        mixed[:, at] = sum(projected(conv_all, slice(HD, PAIR), at, h) for h in range(0, 2 * n_fs, 2))

    kept = (seq_x == x) & (my_owner == c)
    sent_all = (seq_x != x) | (my_owner != c)
    for h in range(0, 2 * n_fs, 2):
        here_too = kept & (head // 2 == h // 2)
        not_here = sent_all | (head // 2 != h // 2)

        @pl.when(here_too)
        def _():
            together(o_recv.at[h // 2], (2 * own_seqs - 1) * out_size).wait_recv()

        @pl.when(not_here)
        def _():
            together(o_recv.at[h // 2], 2 * own_seqs * out_size).wait_recv()

        if h < 2 * n_fs - 2:

            @pl.loop(0, width // columns)
            def _(n):
                at = column(n)
                mixed[:, at] += projected(attn_all, slice(0, HD), at, h)

    @pl.loop(0, width // columns)
    def _(n):
        at = column(n)
        total = mixed[:, at] + projected(attn_all, slice(0, HD), at, 2 * n_fs - 2)
        for s in range(own_seqs):
            out_ref[s, :, at] = total[s * rows : (s + 1) * rows].astype(BF16)

    together(send.at[0], 12 * shard_size).wait_send()
    together(send.at[1], 7 * token_size).wait_send()
    together(send.at[2], (n_sp - 1) * slice_size * 2).wait_send()
    together(send.at[3], (2 * n_sp - 1) * slice_size).wait_send()
    together(send.at[4], last * block * 6 * HD).wait_send()
    together(send.at[5], 7 * width * 2 * PAIR).wait_send()
    together(send.at[6], len(conv_to) * conv_size).wait_send()
    together(send.at[7], n_seq * kv_size).wait_send()
    lam_copy.wait_send()
    tail_copy.wait_send()

    @pl.when(away)
    def _():
        qkv_copy(last, 0).wait_send()

    @pl.when(kept)
    def _():
        together(send.at[8], (2 * n_seq - 1) * out_size).wait_send()

    @pl.when(sent_all)
    def _():
        together(send.at[8], 2 * n_seq * out_size).wait_send()


def on_device(n_grp, n_sp, n_fs, *args):
    tokens, norm_gain, wq, wk, wv, q_gain, k_gain, lam, head_gain, wb, wc, wi, taps, woa, woc = args
    own_seqs, rows, width = tokens.shape
    n_seq, block, n_head = own_seqs * n_fs, 2 * rows, 2 * n_fs
    assert n_grp % 2 == 0 and n_sp == 2 * n_seq and n_fs == 4 and own_seqs == 2
    half_ring = n_sp // 2
    row = lambda v: v.reshape(1, -1)
    ins = (
        tokens, row(norm_gain), wq, wk, wv, row(q_gain), row(k_gain), row(lam), row(head_gain),
        wb, wc, wi, taps, woa.T, woc.T,
    )
    dma = pltpu.SemaphoreType.DMA
    vmem = pl.BlockSpec(memory_space=pltpu.VMEM)
    call = pl.pallas_call(
        functools.partial(kernel, n_grp, n_sp, n_fs),
        out_shape=jax.ShapeDtypeStruct(tokens.shape, BF16),
        in_specs=[pl.BlockSpec(memory_space=pltpu.HBM)] * 15,
        out_specs=vmem,
        scratch_shapes=[pltpu.VMEM(a.shape, a.dtype) for a in ins]
        + [
            pltpu.VMEM((n_fs, 2 * own_seqs * rows, width), BF16),
            pltpu.VMEM((n_fs, 4, wq.shape[0], PAIR), BF16),
            pltpu.VMEM((3 + n_head, width, PAIR), BF16),
            pltpu.VMEM((2, n_fs, 2 * own_seqs * rows, PAIR), F32),
            pltpu.VMEM((n_seq, block, 3 * HD), BF16),
            pltpu.VMEM((n_fs, 2 * own_seqs * rows, HD), BF16),
            pltpu.VMEM((n_sp, block, 3 * HD), BF16),
            pltpu.VMEM((2 * block, n_sp * block * 3 // 2), F32),
            pltpu.VMEM((n_seq, block, HD), BF16),
            pltpu.VMEM((n_head, own_seqs * rows, HD), BF16),
            pltpu.VMEM((n_seq, TAIL + block, HD), F32),
            pltpu.VMEM((n_head, own_seqs * rows, HD), BF16),
            pltpu.VMEM((n_head, own_seqs * rows, HD), BF16),
            pltpu.VMEM((2, 8, HD), F32),
            pltpu.VMEM((own_seqs * rows, width), F32),
            dma((10,)),
            dma((4,)),
            dma((1, 5)),
            dma((2, half_ring, 5)),
            dma((7,)),
            pltpu.SemaphoreType.REGULAR,
            dma((n_seq,)),
            dma((1,)),
            dma((n_fs,)),
            dma((1,)),
            dma((4, 5)),
            dma((2,)),
            dma((2,)),
            dma((8,)),
        ],
        compiler_params=pltpu.CompilerParams(
            collective_id=0, has_side_effects=True, vmem_limit_bytes=32 * 1024 * 1024
        ),
    )
    return call(*[pltpu.with_memory_space_constraint(a, pltpu.HBM) for a in ins])


def solution(mesh):
    placed = (
        P(("grp", "fs"), ("sp", "tp"), None),
        P(),
        P(("sp", "fs"), "tp"),
        P(("sp", "fs"), "tp"),
        P(("sp", "fs"), "tp"),
        P("tp"),
        P("tp"),
        P("tp"),
        P(),
        P(("sp", "fs"), "tp"),
        P(("sp", "fs"), "tp"),
        P(("sp", "fs"), "tp"),
        P(None, "tp"),
        P("tp", ("sp", "fs")),
        P("tp", ("sp", "fs")),
    )
    return jax.shard_map(
        functools.partial(on_device, mesh.shape["grp"], mesh.shape["sp"], mesh.shape["fs"]),
        mesh=mesh,
        in_specs=placed,
        out_specs=P(("grp", "fs"), ("sp", "tp"), None),
        check_vma=False,
    )
```

```python
import functools

import jax
import jax.numpy as jnp
from jax import lax
from jax.experimental import pallas as pl
from jax.experimental.pallas import tpu as pltpu
from jax.sharding import PartitionSpec as P

EPS = 1e-06
NEG = -1e30
OUT_SCALE = 0.8
HD = 128
HALF = HD // 2
PAIR = 2 * HD
TAIL = 8
F32 = jnp.float32
BF16 = jnp.bfloat16
MESH = pl.DeviceIdType.MESH


def kernel(
    n_grp,
    n_sp,
    n_fs,
    *refs,
):
    (tok_ref, norm_gain_ref, wq_ref, wk_ref, wv_ref, q_gain_ref, k_gain_ref, lam_ref, head_gain_ref, wb_ref, wc_ref, wi_ref, taps_ref, woa_ref, woc_ref) = refs[16:31]
    (
    out_ref,
    tokens,
    stage,
    wall,
    partial,
    qkv,
    gate_b,
    heads,
    score,
    attn,
    attn_all,
    shaped,
    conv,
    conv_all,
    lams,
    mixed,
    send,
    w_recv,
    t_recv,
    ring_recv,
    pair_recv,
    ready,
    pace,
    a_recv,
    kv_recv,
    o_recv,
    c_recv,
    wo_recv,
    one_send,
    one_recv,
    load_sem,
    ) = (refs[15], *refs[31:])
    weights, others = (2, 3, 4, 9, 10, 11, 13, 14), (0, 1, 5, 6, 7, 8, 12)
    load_at = {n: 0 for n in weights} | {n: 1 + i for i, n in enumerate(others)}
    loads = [pltpu.make_async_copy(refs[n], refs[16 + n], load_sem.at[load_at[n]]) for n in range(15)]
    for n in weights + others:
        loads[n].start()
    g = lax.axis_index("grp")
    z, x, c = lax.axis_index("sp"), lax.axis_index("fs"), lax.axis_index("tp")
    own_seqs, rows, width = tok_ref.shape
    own_rows = own_seqs * rows
    block = 2 * rows
    keys = 2 * block
    part = wq_ref.shape[0]
    zpart = n_fs * part
    n_seq = own_seqs * n_fs
    half_ring = n_sp // 2
    xr, xl, xo = lax.rem(x + 1, n_fs), lax.rem(x + n_fs - 1, n_fs), lax.rem(x + 2, n_fs)
    zr, zl = lax.rem(z + 1, n_sp), lax.rem(z + n_sp - 1, n_sp)
    other = 1 - c
    me = n_fs * c + x
    odd = lax.rem(g, 2)
    pair = g + 1 - 2 * odd
    out_at = 3

    def copy(src, dst, send, recv, **where):
        return pltpu.make_async_remote_copy(
            src_ref=src,
            dst_ref=dst,
            send_sem=send,
            recv_sem=recv,
            device_id=where,
            device_id_type=MESH,
        )

    def together(sem, size):
        lines = size // (2 * PAIR)
        for most in range(1, wall.shape[0] + 1):
            if lines % most == 0 and lines // most <= width and lines // most % 16 == 0:
                ref = wall.at[0:most, 0 : lines // most, :]
                return copy(ref, ref, sem, sem, tp=other)
        raise ValueError(size)

    shard_size, slice_size = part * 2 * PAIR, zpart * 2 * PAIR
    token_size, conv_size = own_rows * width * 2, own_rows * HD * 2
    out_size, kv_size = rows * HD * 2, block * 2 * PAIR

    barrier = pltpu.get_barrier_semaphore()
    near = [dict(fs=xr), dict(fs=xl), dict(fs=xo), dict(tp=other), dict(sp=zl), dict(grp=pair)]
    for where in near:
        pl.semaphore_signal(barrier, inc=1, device_id=where, device_id_type=MESH)

    pltpu.make_async_copy(stage, stage, load_sem.at[0]).wait()
    for n in others:
        loads[n].wait()

    sides = ((wq_ref, wk_ref), (wv_ref, wb_ref), (wc_ref, wi_ref), (woa_ref, woc_ref))
    for to in range(n_fs):
        lanes = slice(to * HD, (to + 1) * HD)
        for k, (left, right) in enumerate(sides):
            stage[to, k, :, 0:HD] = left[:, lanes]
            stage[to, k, :, HD:PAIR] = right[:, lanes]
    pl.semaphore_wait(barrier, len(near))

    pl.semaphore_signal(ready, inc=1, device_id=dict(sp=zr), device_id_type=MESH)

    def chunk_at(k, to):
        return out_at + n_fs * c + to if k == 3 else k

    def shard_copy(k, n, to, source):
        at = pl.ds(pl.multiple_of(z * zpart + source * part, part), part)
        return copy(stage.at[to, k], wall.at[chunk_at(k, to), at, :], send.at[0], w_recv.at[k], fs=to)

    for k in range(4):
        for n, to in ((2, xo), (0, xr), (1, xl)):
            shard_copy(k, n, to, x).start()
    here = pl.ds(pl.multiple_of(z * zpart + x * part, part), part)
    wall[0:3, here, :] = stage[x, 0:3]
    wall[out_at + me, here, :] = stage[x, 3]

    step_rows = min(rows, 32)
    for s in range(own_seqs):
        for r in range(0, rows, step_rows):
            wide = tok_ref[s, r : r + step_rows, :].astype(F32)
            scale = lax.rsqrt(jnp.mean(wide * wide, axis=-1, keepdims=True) + EPS)
            at = pl.multiple_of(c * own_rows + s * rows + r, step_rows)
            tokens[x, pl.ds(at, step_rows), :] = (wide * scale * norm_gain_ref[...]).astype(BF16)

    class RowGather:
        def __init__(self, ref, size, send, recv, j):
            self.ref, self.size, self.send, self.recv, self.j = ref, size, send, recv, j

        def one(self, n, i, part_of, **where):
            first, length = ((0, self.size), (0, self.size // 2), (self.size // 2, self.size // 2))[part_of]
            ref = self.ref(i, first, length)
            return copy(ref, ref, self.send, self.recv.at[self.j if n < 4 else 0, min(n, 4)], **where)

        def sent_as(self, n):
            i, part_of, where = (
                (x, 0, dict(fs=xr)),
                (x, 0, dict(fs=xl)),
                (xl, 1, dict(fs=xr)),
                (xr, 2, dict(fs=xl)),
                (x, 0, dict(tp=other)),
                (xl, 0, dict(tp=other)),
                (xr, 0, dict(tp=other)),
                (xo, 0, dict(tp=other)),
            )[n]
            return self.one(n, i, part_of, **where)

        def own(self):
            for n in (0, 1, 4):
                self.sent_as(n).start()

        def neighbours(self):
            self.one(0, xl, 0, fs=xr).wait_recv()
            self.sent_as(2).start()
            self.one(1, xr, 0, fs=xl).wait_recv()
            for n in (3, 5, 6):
                self.sent_as(n).start()

        def opposite(self):
            self.one(2, xo, 1, fs=xr).wait_recv()
            self.one(3, xo, 2, fs=xl).wait_recv()
            self.sent_as(7).start()

    def token_ref(core):
        def ref(i, first, length):
            return tokens.at[i, pl.ds(pl.multiple_of(core * own_rows + first, length), length), :]

        return ref

    token_gather = RowGather(token_ref(c), own_rows, send.at[1], t_recv, 0)

    lane = lax.broadcasted_iota(jnp.int32, lam_ref.shape, 1)
    chosen = jnp.sum(jnp.where(lane == x, lam_ref[...], 0.0), axis=-1, keepdims=True)
    lams[c] = jnp.broadcast_to(chosen, lams.shape[1:])
    lam_copy = copy(lams.at[c], lams.at[c], one_send.at[0], one_recv.at[0], tp=other)
    lam_copy.start()

    pieces_of = ((0, 0), (1, 0), (2, 0), (2, 1), (3, 0))

    def slice_ref(k, zb, side):
        kind, nth = pieces_of[k]
        length = zpart // 2
        at = pl.ds(pl.multiple_of(zb * zpart + (nth if kind == 2 else side) * length, length), length)
        if kind == 2:
            return wall.at[2 + side * (1 + me), at, :]
        return wall.at[(0, 1, 2, 1)[kind], at, (slice(0, PAIR), slice(0, HD), None, slice(HD, PAIR))[kind]]

    def ring_block(way, step):
        return lax.rem(z - step + 2 * n_sp, n_sp) if way == 0 else lax.rem(z + step, n_sp)

    def ring(way, step, k, ahead):
        ref = slice_ref(k, ring_block(way, step + ahead), odd)
        to = zr if way == 0 else zl
        return copy(ref, ref, send.at[2], ring_recv.at[way, step, k], sp=to)

    soon = half_ring - 3

    def pair_copy(way, step, k, side):
        ref = slice_ref(k, ring_block(way, step + 1), side)
        recv = pair_recv.at[6 if k == 4 else 0 if step < soon else 1]
        return copy(ref, ref, send.at[3], recv, grp=pair)

    pieces = wo_recv.shape[0]
    piece = width // pieces

    def pair_piece(j, side):
        ref = wall.at[2 + side * (1 + me), pl.ds(j * piece, piece), :]
        return copy(ref, ref, send.at[3], pair_recv.at[2 + j], grp=pair)

    def active(way, step, k):
        return step < half_ring - 1 or (step == half_ring - 1 and (k in (0, 2)) == (way == 0))

    @pl.when(z != 0)
    def _():
        pl.semaphore_wait(ready, 1)

    for k in range(4):
        together(w_recv.at[k], 3 * shard_size).wait_recv()
        for slot, its in enumerate((0, 1, 3, 3, 1)):
            if k == its:
                ring(0, 0, slot, 0).start()

                @pl.when(z != 0)
                def _():
                    ring(1, 0, slot, 0).start()

    token_gather.own()
    @pl.when(z == 0)
    def _():
        pl.semaphore_wait(ready, 1)
        for k in range(5):
            ring(1, 0, k, 0).start()

    def project(i, blocks, first=False):
        for k in range(2):
            lanes = slice(0, PAIR if k == 0 else HD)
            total = None if first else partial[k, i, :, lanes]
            for zb in blocks:
                at = pl.ds(pl.multiple_of(zb * zpart, zpart), zpart)
                add = jnp.dot(tokens[i, :, at], wall[k, at, lanes], preferred_element_type=F32)
                total = add if total is None else total + add
            partial[k, i, :, lanes] = total

    def blocks_of(steps):
        return [ring_block(way, step + 1) for step in steps for way in range(2)]

    for step in range(half_ring):
        if step >= 2:

            @pl.when(c == 1)
            def _():
                pl.semaphore_wait(pace, 1)

        for k in range(5):
            for way in range(2):
                if active(way, step, k):
                    ring(way, step, k, 1).wait_recv()
                    if active(way, step + 1, k):
                        ring(way, step + 1, k, 0).start()
                    if k < 2:
                        pair_copy(way, step, k, odd).start()
        if step < half_ring - 2:

            @pl.when(c == 0)
            def _():
                pl.semaphore_signal(pace, inc=1, device_id=dict(tp=other), device_id_type=MESH)

        if step == half_ring // 2:
            token_gather.neighbours()
        if step == half_ring - 2:
            token_gather.opposite()
    together(pair_recv.at[0], 2 * soon * slice_size * 3 // 4).wait_recv()
    for j in range(pieces):
        pair_piece(j, odd).start()
    for step in range(half_ring):
        for way in range(2):
            if active(way, step, 4):
                pair_copy(way, step, 4, odd).start()
    together(t_recv.at[0, 4], n_fs * token_size).wait_recv()
    for i in range(n_fs):
        project(i, [z] + blocks_of(range(soon)), first=True)
    together(pair_recv.at[1], (n_sp - 1 - 2 * soon) * slice_size * 3 // 4).wait_recv()
    last_blocks = blocks_of(range(soon, half_ring - 1)) + [ring_block(0, half_ring)]

    def w_out_ref(core, j):
        def ref(i, first, length):
            return wall.at[out_at + n_fs * core + i, pl.ds(j * piece + first, length), :]

        return ref

    w_out_gathers = [RowGather(w_out_ref(c, j), piece, send.at[5], wo_recv, j) for j in range(pieces)]

    lanes_x = pl.ds(pl.multiple_of(x * HD, HD), HD)
    low = lax.broadcasted_iota(jnp.int32, (2 * own_rows, HD), 1) < HALF

    def unit(raw, gain):
        wide = raw.astype(BF16).astype(F32)
        square = wide * wide
        first = jnp.sum(jnp.where(low, square, 0.0), axis=-1, keepdims=True)
        second = jnp.sum(jnp.where(low, 0.0, square), axis=-1, keepdims=True)
        scale = jnp.where(low, lax.rsqrt(first / HALF + EPS), lax.rsqrt(second / HALF + EPS))
        return wide * scale * gain

    for i in range(n_fs):
        project(i, last_blocks)
        both = partial[0, i]
        query = (unit(both[:, :HD], q_gain_ref[:, lanes_x]) * HALF**-0.5).astype(BF16)
        key = unit(both[:, HD:], k_gain_ref[:, lanes_x]).astype(BF16)
        value = partial[1, i, :, 0:HD].astype(BF16)
        for s in range(own_seqs):
            for core in range(2):
                src = slice(core * own_rows + s * rows, core * own_rows + (s + 1) * rows)
                dst = slice(core * rows, (core + 1) * rows)
                qkv[own_seqs * i + s, dst, 0:HD] = query[src]
                qkv[own_seqs * i + s, dst, HD:PAIR] = key[src]
                qkv[own_seqs * i + s, dst, PAIR:] = value[src]

    def owner(zb):
        return lax.rem(lax.rem(zb, 2) + zb // 2, 2)

    def own_block(i):
        return 2 * i + lax.rem(i + c, 2)

    def other_block(i):
        return 2 * i + lax.rem(i + other, 2)

    offsets = [n_seq // 2]
    for d in range(n_seq // 2 - 1, 0, -1):
        offsets += [d, n_seq - d]
    my_owner = owner(z)

    last = len(offsets)

    def qkv_copy(n, offset):
        s = lax.rem(z // 2 + offset, n_seq)
        return copy(qkv.at[s], heads.at[z], send.at[4 if n < last else 9], a_recv.at[z // 2], sp=2 * s + c, tp=my_owner)

    for n, offset in enumerate(offsets):
        qkv_copy(n, offset).start()
    home = (c == lax.rem(z, 2)) & (my_owner == c)
    away = (c != lax.rem(z, 2)) | (my_owner != c)

    @pl.when(away)
    def _():
        qkv_copy(last, 0).start()

    @pl.when(home)
    def _():
        heads[z] = qkv[z // 2]

    for j, gather in enumerate(w_out_gathers):
        together(pair_recv.at[2 + j], piece * 2 * PAIR).wait_recv()
        gather.own()
    together(pair_recv.at[6], (n_sp - 1) * slice_size // 4).wait_recv()

    @pl.loop(0, n_fs)
    def _(i):
        both = jnp.dot(tokens[i], wall[2], preferred_element_type=F32).astype(BF16)
        both = both.astype(F32)
        gate_b[i] = jnp.dot(tokens[i], wall[1, :, HD:PAIR], preferred_element_type=F32).astype(BF16)
        product = (both[:, :HD] * both[:, HD:]).astype(BF16).astype(F32)
        for s in range(own_seqs):
            for core in range(2):
                src = slice(core * own_rows + s * rows, core * own_rows + (s + 1) * rows)
                shaped[own_seqs * i + s, TAIL + core * rows : TAIL + (core + 1) * rows, :] = product[src]

    tail_copy = copy(
        shaped.at[:, block : block + TAIL, :],
        shaped.at[:, 0:TAIL, :],
        one_send.at[1],
        one_recv.at[1],
        sp=zr,
    )
    tail_copy.start()
    for gather in w_out_gathers:
        gather.neighbours()

    def kv_copy(i, zb):
        ref = heads.at[zb, :, HD:]
        return copy(ref, ref, send.at[7], kv_recv.at[0], tp=other)

    for i in range(n_seq):
        zb = own_block(i)

        @pl.when((zb != z) | (c != lax.rem(z, 2)))
        def _():
            copy(qkv.at[0], heads.at[zb], send.at[4], a_recv.at[i], sp=zb, tp=c).wait_recv()

        kv_copy(i, zb).start()
    tail_copy.wait_recv()

    @pl.when(z == 0)
    def _():
        shaped[:, 0:TAIL, :] = jnp.zeros((n_seq, TAIL, HD), F32)

    taps = [taps_ref[i : i + 1, lanes_x] for i in range(3)]

    @pl.loop(0, n_fs)
    def _(i):
        for s in range(own_seqs):
            seq = own_seqs * i + s
            total = taps[0] * shaped[seq, TAIL - 2 : TAIL - 2 + block, :]
            total = total + taps[1] * shaped[seq, TAIL - 1 : TAIL - 1 + block, :]
            total = total + taps[2] * shaped[seq, TAIL : TAIL + block, :]
            for core in range(2):
                gate = gate_b[i, core * own_rows + s * rows : core * own_rows + (s + 1) * rows, :]
                gated = gate.astype(F32) * total[core * rows : (core + 1) * rows]
                conv[2 * i + core, s * rows : (s + 1) * rows, :] = gated.astype(BF16)

    def conv_copy(n, to, core):
        return copy(conv.at[2 * to + core], conv_all.at[me], send.at[6], c_recv.at[0], fs=to, tp=core)

    conv_to = [(xo, c), (xo, other), (xr, c), (xr, other), (xl, c), (xl, other), (x, other)]
    for n, (to, core) in enumerate(conv_to):
        conv_copy(n, to, core).start()
    conv_all[me] = conv[2 * x + c]


    for gather in w_out_gathers[:-1]:
        gather.opposite()
    lam_copy.wait_recv()
    together(kv_recv.at[0], n_seq * kv_size).wait_recv()

    seq, mine = z // 2, lax.rem(z, 2)
    head = n_fs * mine + x
    seq_x, seq_row = seq // own_seqs, pl.ds(pl.multiple_of(lax.rem(seq, own_seqs) * rows, rows), rows)
    lane = lax.broadcasted_iota(jnp.int32, (block, HD), 1)
    key_at = lax.broadcasted_iota(jnp.int32, (2 * block, keys), 1)
    row_at = lax.rem(lax.broadcasted_iota(jnp.int32, (2 * block, keys), 0), block)

    def out_copy(i, zb, core):
        return copy(
            attn.at[i, core * rows : (core + 1) * rows, :],
            attn_all.at[head, seq_row, :],
            send.at[8],
            o_recv.at[head // 2],
            fs=seq_x,
            sp=zb,
            tp=core,
        )

    def is_self(zb, core):
        return (seq_x == x) & (zb == z) & (c == core)

    def not_self(zb, core):
        return (seq_x != x) | (zb != z) | (c != core)

    def scored(i, first):
        zb = own_block(i)
        query = heads[zb, :, 0:HD].astype(F32)
        query = jnp.concatenate(
            [jnp.where(lane < HALF, query, 0.0), jnp.where(lane < HALF, 0.0, query)], axis=0
        ).astype(BF16)
        top = None
        for j in range(i + 1):
            key = heads[2 * j : 2 * j + 2, :, HD:PAIR].reshape(keys, HD)
            s = lax.dot_general(query, key, (((1,), (1,)), ((), ())), preferred_element_type=F32)
            if j == i:
                s = jnp.where(key_at <= row_at + block * lax.rem(i + c, 2), s, NEG)
            score[:, first + j * keys : first + (j + 1) * keys] = s
            top = folded(jnp.maximum, s, top)
        return jnp.max(top, axis=-1, keepdims=True)

    def folded(op, s, start):
        for n in range(0, keys, min(HD, keys)):
            piece = s[:, n : n + min(HD, keys)]
            start = piece if start is None else op(start, piece)
        return start

    def weighted(i, first, top):
        total, summed = None, None
        for j in range(i + 1):
            weight = jnp.exp(score[:, first + j * keys : first + (j + 1) * keys] - top)
            value = heads[2 * j : 2 * j + 2, :, PAIR:].reshape(keys, HD)
            add = jnp.dot(weight.astype(BF16), value, preferred_element_type=F32)
            total = folded(jnp.add, weight, total)
            summed = add if summed is None else summed + add
        return summed, jnp.sum(total, axis=-1, keepdims=True)

    def finished(i, summed, total):
        maps = summed / total
        differ = maps[:block] - lams[mine][0:1, :] * maps[block:]
        scale = lax.rsqrt(jnp.mean(differ * differ, axis=-1, keepdims=True) + EPS)
        attn[i] = (differ * scale * head_gain_ref[...] * OUT_SCALE).astype(BF16)

    def deliver(i):
        zb = own_block(i)
        for core in range(2):

            @pl.when(not_self(zb, core))
            def _():
                out_copy(i, zb, core).start()

            @pl.when(is_self(zb, core))
            def _():
                attn_all[head, seq_row, :] = attn[i, core * rows : (core + 1) * rows, :]

    side = jnp.minimum(seq, n_seq - 1 - seq)

    @pl.loop(0, n_seq // 2)
    def _(turn):
        late_turn = turn // 2
        inner = side // 2
        first = n_seq // 2 - 1 - side
        now = (1 - late_turn) * (first + lax.rem(turn, 2) * (1 - 2 * lax.rem(first, 2))) + late_turn * (
            inner * turn + (1 - inner) * (n_seq // 2 - 1 - turn)
        )
        for p in range(n_seq // 2):

            @pl.when(now == p)
            def _():
                both = ((n_seq - 1 - p, 0), (p, n_sp * block))
                tops = [scored(i, first) for i, first in both]
                sums = [weighted(i, first, top) for (i, first), top in zip(both, tops)]
                for (i, _), (summed, total) in zip(both, sums):
                    finished(i, summed, total)
                for i, _ in both:
                    deliver(i)

    w_out_gathers[-1].opposite()
    together(wo_recv.at[0, 4], n_fs * width * 2 * PAIR).wait_recv()
    together(c_recv.at[0], len(conv_to) * conv_size).wait_recv()
    columns = min(width, 256)

    def projected(features, lanes, at, h):
        weight = jnp.concatenate([wall[out_at + h, at, lanes], wall[out_at + h + 1, at, lanes]], axis=1)
        pair_of = jnp.concatenate([features[h], features[h + 1]], axis=1)
        return lax.dot_general(pair_of, weight, (((1,), (1,)), ((), ())), preferred_element_type=F32)

    def column(n):
        return pl.ds(pl.multiple_of(n * columns, columns), columns)

    @pl.loop(0, width // columns)
    def _(n):
        at = column(n)
        mixed[:, at] = sum(projected(conv_all, slice(HD, PAIR), at, h) for h in range(0, 2 * n_fs, 2))

    kept = (seq_x == x) & (my_owner == c)
    sent_all = (seq_x != x) | (my_owner != c)
    for h in range(0, 2 * n_fs, 2):
        here_too = kept & (head // 2 == h // 2)
        not_here = sent_all | (head // 2 != h // 2)

        @pl.when(here_too)
        def _():
            together(o_recv.at[h // 2], (2 * own_seqs - 1) * out_size).wait_recv()

        @pl.when(not_here)
        def _():
            together(o_recv.at[h // 2], 2 * own_seqs * out_size).wait_recv()

        if h < 2 * n_fs - 2:

            @pl.loop(0, width // columns)
            def _(n):
                at = column(n)
                mixed[:, at] += projected(attn_all, slice(0, HD), at, h)

    @pl.loop(0, width // columns)
    def _(n):
        at = column(n)
        total = mixed[:, at] + projected(attn_all, slice(0, HD), at, 2 * n_fs - 2)
        for s in range(own_seqs):
            out_ref[s, :, at] = total[s * rows : (s + 1) * rows].astype(BF16)

    together(send.at[0], 12 * shard_size).wait_send()
    together(send.at[1], 7 * token_size).wait_send()
    together(send.at[2], (n_sp - 1) * slice_size * 2).wait_send()
    together(send.at[3], (2 * n_sp - 1) * slice_size).wait_send()
    together(send.at[4], last * block * 6 * HD).wait_send()
    together(send.at[5], 7 * width * 2 * PAIR).wait_send()
    together(send.at[6], len(conv_to) * conv_size).wait_send()
    together(send.at[7], n_seq * kv_size).wait_send()
    lam_copy.wait_send()
    tail_copy.wait_send()

    @pl.when(away)
    def _():
        qkv_copy(last, 0).wait_send()

    @pl.when(kept)
    def _():
        together(send.at[8], (2 * n_seq - 1) * out_size).wait_send()

    @pl.when(sent_all)
    def _():
        together(send.at[8], 2 * n_seq * out_size).wait_send()


def on_device(n_grp, n_sp, n_fs, *args):
    tokens, norm_gain, wq, wk, wv, q_gain, k_gain, lam, head_gain, wb, wc, wi, taps, woa, woc = args
    own_seqs, rows, width = tokens.shape
    n_seq, block, n_head = own_seqs * n_fs, 2 * rows, 2 * n_fs
    assert n_grp % 2 == 0 and n_sp == 2 * n_seq and n_fs == 4 and own_seqs == 2
    half_ring = n_sp // 2
    row = lambda v: v.reshape(1, -1)
    ins = (
        tokens, row(norm_gain), wq, wk, wv, row(q_gain), row(k_gain), row(lam), row(head_gain),
        wb, wc, wi, taps, woa.T, woc.T,
    )
    dma = pltpu.SemaphoreType.DMA
    vmem = pl.BlockSpec(memory_space=pltpu.VMEM)
    call = pl.pallas_call(
        functools.partial(kernel, n_grp, n_sp, n_fs),
        out_shape=jax.ShapeDtypeStruct(tokens.shape, BF16),
        in_specs=[pl.BlockSpec(memory_space=pltpu.HBM)] * 15,
        out_specs=vmem,
        scratch_shapes=[pltpu.VMEM(a.shape, a.dtype) for a in ins]
        + [
            pltpu.VMEM((n_fs, 2 * own_seqs * rows, width), BF16),
            pltpu.VMEM((n_fs, 4, wq.shape[0], PAIR), BF16),
            pltpu.VMEM((3 + n_head, width, PAIR), BF16),
            pltpu.VMEM((2, n_fs, 2 * own_seqs * rows, PAIR), F32),
            pltpu.VMEM((n_seq, block, 3 * HD), BF16),
            pltpu.VMEM((n_fs, 2 * own_seqs * rows, HD), BF16),
            pltpu.VMEM((n_sp, block, 3 * HD), BF16),
            pltpu.VMEM((2 * block, n_sp * block * 3 // 2), F32),
            pltpu.VMEM((n_seq, block, HD), BF16),
            pltpu.VMEM((n_head, own_seqs * rows, HD), BF16),
            pltpu.VMEM((n_seq, TAIL + block, HD), F32),
            pltpu.VMEM((n_head, own_seqs * rows, HD), BF16),
            pltpu.VMEM((n_head, own_seqs * rows, HD), BF16),
            pltpu.VMEM((2, 8, HD), F32),
            pltpu.VMEM((own_seqs * rows, width), F32),
            dma((10,)),
            dma((4,)),
            dma((1, 5)),
            dma((2, half_ring, 5)),
            dma((7,)),
            pltpu.SemaphoreType.REGULAR,
            pltpu.SemaphoreType.REGULAR,
            dma((n_seq,)),
            dma((1,)),
            dma((n_fs,)),
            dma((1,)),
            dma((4, 5)),
            dma((2,)),
            dma((2,)),
            dma((8,)),
        ],
        compiler_params=pltpu.CompilerParams(
            collective_id=0, has_side_effects=True, vmem_limit_bytes=32 * 1024 * 1024
        ),
    )
    return call(*[pltpu.with_memory_space_constraint(a, pltpu.HBM) for a in ins])


def solution(mesh):
    placed = (
        P(("grp", "fs"), ("sp", "tp"), None),
        P(),
        P(("sp", "fs"), "tp"),
        P(("sp", "fs"), "tp"),
        P(("sp", "fs"), "tp"),
        P("tp"),
        P("tp"),
        P("tp"),
        P(),
        P(("sp", "fs"), "tp"),
        P(("sp", "fs"), "tp"),
        P(("sp", "fs"), "tp"),
        P(None, "tp"),
        P("tp", ("sp", "fs")),
        P("tp", ("sp", "fs")),
    )
    return jax.shard_map(
        functools.partial(on_device, mesh.shape["grp"], mesh.shape["sp"], mesh.shape["fs"]),
        mesh=mesh,
        in_specs=placed,
        out_specs=P(("grp", "fs"), ("sp", "tp"), None),
        check_vma=False,
    )
```
